512 devices in a mesh: pp: 16 (over y, x), tp: 32 (over z, core).
Axes of the slice: x: 4, y: 4, z: 16, core: 2. Of those that a mesh axis runs over, the one named last changes fastest.
Arguments:
- entry_stream_rows: bfloat16 [1024, 2048], P('pp', 'tp'), may hold values from -21 to 21
- layer_rescale_factor: float32 [16, 2048], P('pp'), may hold values from 0.1 to 1.9
- probe_projection: bfloat16 [16, 2048, 2048], P('pp', 'tp'), may hold values from -0.125 to 0.125
- retention_projection: bfloat16 [16, 2048, 2048], P('pp', 'tp'), may hold values from -0.125 to 0.125
- candidate_projection: bfloat16 [16, 2048, 2048], P('pp', 'tp'), may hold values from -0.125 to 0.125
- emission_filter_matrix: bfloat16 [16, 2048, 2048], P('pp', 'tp'), may hold values from -0.125 to 0.125
- retention_minimum: float32 [16, 2048], P('pp', 'tp'), may hold values from 0.88 to 0.9921875
- decay_spike: float32 [16, 128, 32], P('pp', None, 'tp'), may hold values from -2.1 to 0
- per_group_scale: float32 [16, 64], P('pp'), may hold values from 0.1 to 1.9
Outputs:
- outputs: bfloat16 [1024, 2048], P('pp', 'tp')
The draws below stay inside these ranges and needn't reach their ends.
All inputs are finite; a program needn't handle non-finite values.
Results may differ from the reference program's by a relative error of at most 0.03.
Values may be sent and summed in bfloat16 or wider, within the bound.
No kernel may reach another device: no remote copies, remote signals or barrier semaphores. Data moves between devices by JAX's collectives and lax.ppermute only.
A program may use at most 64 MiB of HBM per device.

```python
import math
import jax
import jax.numpy as jnp
from jax import lax

HEADS = 32
HEAD = 64
D = 2048
SEG = 64
MB_TOK = 128
SECTIONS = 16
MICRO = 8


def draw_entry_stream_rows(key, part):
    first_key, second_key, third_key = jax.random.split(jax.random.fold_in(key, 11), 3)
    rows = MICRO * MB_TOK
    column = jnp.arange(D, dtype=jnp.float32) / D
    values = jnp.clip(jax.random.normal(first_key, (rows, D), jnp.float32), -4.0, 4.0)
    row_scale = jnp.exp(jax.random.uniform(second_key, (rows, 1), jnp.float32, math.log(0.5), math.log(2.0)))
    rising = 3.0 ** (column - 0.5)
    col_scale = rising[None, :] * jnp.exp(jax.random.uniform(third_key, (1, D), jnp.float32, -0.35, 0.35))
    return (values * row_scale * col_scale).astype(jnp.bfloat16)


def draw_retention_minimum(key, part):
    first_key, second_key, third_key = jax.random.split(jax.random.fold_in(key, 23), 3)
    slow_share = 0.5
    slow_heads = jax.random.uniform(first_key, (SECTIONS, HEADS, 1), jnp.float32) < slow_share
    slow_gap = jnp.exp(jax.random.uniform(second_key, (SECTIONS, HEADS, HEAD), jnp.float32, math.log(1.0 / MB_TOK), math.log(4.0 / MB_TOK)))
    fast_gap = jnp.exp(jax.random.uniform(third_key, (SECTIONS, HEADS, HEAD), jnp.float32, math.log(0.04), math.log(0.12)))
    gap_all = jnp.where(slow_heads, slow_gap, fast_gap)
    return (1.0 - gap_all).reshape(SECTIONS, D).astype(jnp.float32)


def draw_decay_spike(key, part):
    first_key, second_key = jax.random.split(jax.random.fold_in(key, 37), 2)
    where_at = jax.random.randint(first_key, (SECTIONS, 3, HEADS), 0, MB_TOK)
    strength = jnp.log(jax.random.uniform(second_key, (SECTIONS, 3, HEADS), jnp.float32, 0.5, 0.8))
    positions = jnp.arange(MB_TOK, dtype=jnp.int32)[None, :, None, None]
    hit_mask = where_at[:, None, :, :] == positions
    return jnp.sum(jnp.where(hit_mask, strength[:, None, :, :], 0.0), axis=2).astype(jnp.float32)


def steps_of(own_key, shape, cuts, least, top_value):
    gain, own = 1.0, jax.random.fold_in(own_key, 6)
    for dim, blocks in cuts:
        heights = jnp.exp(jax.random.uniform(jax.random.fold_in(own, dim), (blocks,), jnp.float32, least / len(cuts), top_value / len(cuts)))
        gain = gain * jnp.repeat(heights, shape[dim] // blocks).reshape([-1 if axis == dim else 1 for axis in range(len(shape))])
    return gain


def normal_values(key, extent, spread, bound, cuts=(), kind=jnp.bfloat16):
    array = jax.random.normal(key, extent, jnp.float32) * spread
    if len(cuts) > 0:
        array = steps_of(key, extent, cuts, -0.22, 0.18) * array
    return jnp.clip(array, min=-bound, max=bound).astype(kind)


def setup_inputs(seed: int = 0) -> dict:
    keys = jax.random.split(jax.random.key(seed), 10)
    entry_stream_rows = draw_entry_stream_rows(jax.random.fold_in(keys[9], 71), 0)
    layer_rescale_factor = jnp.clip(1.0 + 0.18 * jax.random.normal(keys[1], (SECTIONS, D), jnp.float32), 0.1, 1.9)
    probe_projection = normal_values(keys[2], (SECTIONS, D, D), D ** -0.5, 0.125, ((0, 16), (1, 32)))
    retention_projection = normal_values(keys[3], (SECTIONS, D, D), D ** -0.5, 0.125, ((0, 16), (1, 32)))
    candidate_projection = normal_values(keys[4], (SECTIONS, D, D), D ** -0.5, 0.125, ((0, 16), (1, 32)))
    emission_filter_matrix = normal_values(keys[5], (SECTIONS, D, D), D ** -0.5, 0.125, ((0, 16), (1, 32)))
    retention_minimum = draw_retention_minimum(jax.random.fold_in(keys[9], 71), 0)
    decay_spike = draw_decay_spike(jax.random.fold_in(keys[9], 71), 0)
    per_group_scale = jnp.clip(1.0 + 0.18 * jax.random.normal(keys[8], (SECTIONS, HEAD), jnp.float32), 0.1, 1.9)
    return dict(entry_stream_rows=entry_stream_rows, layer_rescale_factor=layer_rescale_factor, probe_projection=probe_projection, retention_projection=retention_projection, candidate_projection=candidate_projection, emission_filter_matrix=emission_filter_matrix, retention_minimum=retention_minimum, decay_spike=decay_spike, per_group_scale=per_group_scale)


EPSILON = 1e-06
HIGHEST = lax.Precision.HIGHEST

def segment_scan(queries, key_in, log_forget, values, memory):
    head_count = queries.shape[0]
    length = queries.shape[1]
    blocks_count = length // SEG

    def split_blocks(tensor):
        return tensor.reshape(head_count, blocks_count, SEG, tensor.shape[-1]).transpose(1, 0, 2, 3)
    lower_mask = jnp.tril(jnp.ones((SEG, SEG), dtype=bool))[None]

    def one_block(memory_in, pieces):
        block_query, block_key, block_forget, block_value = pieces
        running = jnp.cumsum(block_forget, axis=1)
        query_scaled = block_query * jnp.exp(running)
        key_scaled = block_key * jnp.exp(-running)
        scores = jnp.einsum('hid,hjd->hij', query_scaled, key_scaled, precision=HIGHEST)
        scores = jnp.where(lower_mask, scores, 0.0)
        mixed_out = jnp.einsum('hij,hjv->hiv', scores, block_value, precision=HIGHEST)
        mixed_out = mixed_out + jnp.einsum('hid,hdv->hiv', query_scaled, memory_in, precision=HIGHEST)
        ending = running[:, -1:, :]
        carried_in = jnp.einsum('hjd,hjv->hdv', block_key * jnp.exp(ending - running), block_value, precision=HIGHEST)
        memory_out = jnp.exp(ending[:, 0, :])[:, :, None] * memory_in + carried_in
        return (memory_out, mixed_out)
    memory, mixed_out = lax.scan(one_block, memory, (split_blocks(queries), split_blocks(key_in), split_blocks(log_forget), split_blocks(values)))
    return (mixed_out.transpose(1, 0, 2, 3).reshape(head_count, length, values.shape[-1]), memory)

def head_norm(mixed_out, channel_gain):
    return mixed_out * lax.rsqrt(lax.optimization_barrier(jnp.mean(mixed_out * mixed_out, axis=-1, keepdims=True)) + EPSILON) * channel_gain

def reference(entry_stream_rows, layer_rescale_factor, probe_projection, retention_projection, candidate_projection, emission_filter_matrix, retention_minimum, decay_spike, per_group_scale):
    stream = entry_stream_rows
    for layer_ordinal in range(SECTIONS):
        wide_stream = stream.astype(jnp.float32)
        scaled = (wide_stream * layer_rescale_factor[layer_ordinal][None, :]).astype(jnp.bfloat16)
        inverse = lax.rsqrt(lax.optimization_barrier(jnp.mean(wide_stream * wide_stream, axis=1, keepdims=True)) + EPSILON)

        def per_head(tensor):
            return tensor.reshape(MICRO, MB_TOK, HEADS, HEAD).transpose(0, 2, 1, 3)
        projected = []
        for matrix in (probe_projection, retention_projection, candidate_projection, emission_filter_matrix):
            product = jnp.dot(scaled, matrix[layer_ordinal].T, preferred_element_type=jnp.float32) * inverse
            projected.append(per_head(product))
        query_pre, forget_pre, input_pre, gate_pre = projected
        lower_edge = retention_minimum[layer_ordinal].reshape(1, HEADS, 1, HEAD)
        remaining_portion = decay_spike[layer_ordinal].T[None, :, :, None]
        log_forget = jnp.logaddexp(jnp.log(lower_edge), jnp.log1p(-lower_edge) + jax.nn.log_sigmoid(forget_pre)) + remaining_portion
        key_in = (1.0 - lower_edge) * jax.nn.sigmoid(-forget_pre)
        queries = jax.nn.silu(query_pre)

        def one_sequence(pieces):
            zero_state = jnp.zeros((HEADS, HEAD, HEAD), jnp.float32)
            mixed_seq, final_state = segment_scan(pieces[0], pieces[1], pieces[2], pieces[3], zero_state)
            return mixed_seq
        mixed_out = lax.map(one_sequence, (queries, key_in, log_forget, input_pre))
        branch = head_norm(mixed_out, per_group_scale[layer_ordinal]) * jax.nn.silu(gate_pre)
        branch = branch.transpose(0, 2, 1, 3).reshape(MICRO * MB_TOK, D)
        stream = (wide_stream + branch).astype(jnp.bfloat16)
    return stream
```

```python
import jax
import jax.numpy as jnp
from jax import lax
from jax.experimental import pallas as pl
from jax.experimental.pallas import tpu as pltpu
from jax.sharding import PartitionSpec as P

HEAD = 64
SEG = 64
EPSILON = 1e-06
NT = (((1,), (1,)), ((), ()))
NN = (((1,), (0,)), ((), ()))
TN = (((0,), (0,)), ((), ()))


def section_kernel(flags, got, gain, weights, edge, spike, out_gain, state_in, result, state_out, scaled, inverse):
    pair = pl.program_id(0)
    first, base, core = flags[0], flags[2], flags[3]
    width = got.shape[-1]
    rows = got.shape[1]

    @pl.when(pair == 0)
    def _():
        total = jnp.zeros((rows, 1), jnp.float32)
        for part in range(2):
            wide = got[base + part].astype(jnp.float32)
            columns = pl.ds(part * width, width)
            scaled[:, columns] = (wide * gain[:, columns]).astype(jnp.bfloat16)
            total = total + jnp.sum(wide * wide, axis=1, keepdims=True)
        inverse[...] = jnp.broadcast_to(lax.rsqrt(total / (2 * width) + EPSILON), inverse.shape)

    matrix = weights[...].reshape(8 * HEAD, 2 * width)
    product = lax.dot_general(scaled[...], matrix, NT, preferred_element_type=jnp.float32)
    scale = inverse[...]
    tiles = [product[:, 128 * k : 128 * k + 128] * scale for k in range(4)]
    rolled = [pltpu.roll(tile, HEAD, 1) for tile in tiles]
    low = lax.broadcasted_iota(jnp.int32, (rows, 128), 1) < HEAD
    query_pre = jnp.where(low, tiles[0], rolled[2])
    forget_pre = jnp.where(low, rolled[0], tiles[2])
    values = jnp.where(low, tiles[1], rolled[3]).astype(jnp.bfloat16)
    gate_pre = jnp.where(low, rolled[1], tiles[3])

    lower = edge[0]
    upper = 1.0 - lower
    log_forget = jnp.log(lower + upper * jax.nn.sigmoid(forget_pre)) + spike[0, 0]
    key_in = upper * jax.nn.sigmoid(-forget_pre)
    queries = query_pre * jax.nn.sigmoid(query_pre)

    high = log_forget.astype(jnp.bfloat16)
    rest = (log_forget - high.astype(jnp.float32)).astype(jnp.bfloat16)
    at = lax.broadcasted_iota(jnp.int32, (rows, 2 * rows), 0)
    of = lax.broadcasted_iota(jnp.int32, (rows, 2 * rows), 1)
    of = jnp.where(of >= rows, of - rows, of)
    ones = jnp.where(at >= of, 1.0, 0.0).astype(jnp.bfloat16)
    running = lax.dot_general(ones, jnp.concatenate([high, rest], axis=0), NN, preferred_element_type=jnp.float32)

    query_scaled = queries * jnp.exp(running)
    key_scaled = (key_in * jnp.exp(-running)).astype(jnp.bfloat16)
    stacked = jnp.concatenate(
        [jnp.where(low, query_scaled, 0.0), jnp.where(low, 0.0, query_scaled)], axis=0
    ).astype(jnp.bfloat16)
    scores = lax.dot_general(stacked, key_scaled, NT, preferred_element_type=jnp.float32)
    at = lax.broadcasted_iota(jnp.int32, (2 * rows, rows), 0)
    at = jnp.where(at >= rows, at - rows, at)
    of = lax.broadcasted_iota(jnp.int32, (2 * rows, rows), 1)
    scores = jnp.where(at >= of, scores, 0.0).astype(jnp.bfloat16)
    both = lax.dot_general(scores, values, NN, preferred_element_type=jnp.float32)
    mixed = jnp.where(low, both[:rows], both[rows:])
    state = jnp.where(first == 1, 0.0, state_in[0])
    mixed = mixed + lax.dot_general(
        query_scaled.astype(jnp.bfloat16), state.astype(jnp.bfloat16), NN, preferred_element_type=jnp.float32
    )

    at = lax.broadcasted_iota(jnp.int32, (128, 128), 0) < HEAD
    of = lax.broadcasted_iota(jnp.int32, (128, 128), 1) < HEAD
    same = at == of

    @pl.when(first == 1)
    def _():
        ending = running[rows - 1 :, :]
        kept = (key_in * jnp.exp(ending - running)).astype(jnp.bfloat16)
        carried = lax.dot_general(kept, values, TN, preferred_element_type=jnp.float32)
        state_out[0] = jnp.where(same, carried, 0.0)

    @pl.when(first != 1)
    def _():
        state_out[0] = state_in[0]

    mean = jnp.where(same, 1.0 / HEAD, 0.0).astype(jnp.bfloat16)
    square = mixed * mixed
    high = square.astype(jnp.bfloat16)
    rest = (square - high.astype(jnp.float32)).astype(jnp.bfloat16)
    average = lax.dot_general(high, mean, NN, preferred_element_type=jnp.float32) + lax.dot_general(
        rest, mean, NN, preferred_element_type=jnp.float32
    )
    branch = mixed * lax.rsqrt(average + EPSILON) * out_gain[...] * (gate_pre * jax.nn.sigmoid(gate_pre))
    own = got[base + core, :, pl.ds(pl.multiple_of(pair * 128, 128), 128)].astype(jnp.float32)
    result[...] = (own + branch).astype(jnp.bfloat16)


def section(flags, got, gain, weights, edge, spike, out_gain, state):
    rows, width = got.shape[1:]
    pairs = weights.shape[0] // 2
    return pl.pallas_call(
        section_kernel,
        out_shape=(
            jax.ShapeDtypeStruct((rows, width), jnp.bfloat16),
            jax.ShapeDtypeStruct(state.shape, state.dtype),
        ),
        grid_spec=pltpu.PrefetchScalarGridSpec(
            num_scalar_prefetch=1,
            grid=(pairs,),
            in_specs=[
                pl.BlockSpec(got.shape, lambda g, f: (0, 0, 0)),
                pl.BlockSpec(gain.shape, lambda g, f: (0, 0)),
                pl.BlockSpec((2,) + weights.shape[1:], lambda g, f: (g, 0, 0, 0)),
                pl.BlockSpec((1, 1, 128), lambda g, f: (g, 0, 0)),
                pl.BlockSpec((1, 1, rows, 128), lambda g, f: (f[1], g, 0, 0)),
                pl.BlockSpec((1, 128), lambda g, f: (0, 0)),
                pl.BlockSpec((1, 128, 128), lambda g, f: (g, 0, 0)),
            ],
            out_specs=[
                pl.BlockSpec((rows, 128), lambda g, f: (0, g)),
                pl.BlockSpec((1, 128, 128), lambda g, f: (g, 0, 0)),
            ],
            scratch_shapes=[
                pltpu.VMEM((rows, 2 * width), jnp.bfloat16),
                pltpu.VMEM((rows, 128), jnp.float32),
            ],
        ),
        input_output_aliases={7: 1},
        cost_estimate=pl.CostEstimate(
            flops=2 * rows * weights.size, bytes_accessed=2 * weights.size, transcendentals=0
        ),
    )(flags, got, gain, weights, edge, spike, out_gain, state)


def shards(
    entry_stream_rows,
    layer_rescale_factor,
    probe_projection,
    retention_projection,
    candidate_projection,
    emission_filter_matrix,
    retention_minimum,
    decay_spike,
    per_group_scale,
):
    sections = lax.axis_size("pp")
    members = lax.axis_size("tp")
    chips = members // 2
    layer = lax.axis_index("pp")
    core = lax.axis_index("tp") % 2
    chip = lax.axis_index("tp") // 2
    model_width = layer_rescale_factor.shape[1]
    half_width = model_width // 2
    pairs = chips // 2
    same_core = [[c + 2 * z for z in range(chips)] for c in range(2)]

    def by_core(array):
        split = array.reshape(array.shape[:-1] + (chips, 2, HEAD))
        return jnp.swapaxes(split, -3, -2).reshape(array.shape)

    local = jnp.stack(
        [probe_projection[0], retention_projection[0], candidate_projection[0], emission_filter_matrix[0]]
    )
    weights = lax.all_gather(by_core(local), "tp", axis_index_groups=same_core)
    gain = by_core(layer_rescale_factor)
    small = jnp.concatenate([retention_minimum[0], decay_spike[0, :, 0]])
    small = lax.all_gather(small, "tp", axis_index_groups=same_core)
    edge = small[:, :HEAD].reshape(pairs, 1, 128)
    spike = small[:, HEAD:].reshape(pairs, 2, 2, SEG)
    spike = jnp.broadcast_to(spike.transpose(2, 0, 3, 1)[..., None], (2, pairs, SEG, 2, HEAD))
    spike = spike.reshape(2, pairs, SEG, 128)
    out_gain = jnp.tile(per_group_scale, (1, 2))

    def gathered_line(block):
        whole = lax.all_gather(block, "tp", axis_index_groups=same_core)
        return whole.transpose(1, 0, 2).reshape(block.shape[0], half_width)

    def between(array, pairs_of):
        moves = [
            (a * members + t, b * members + t)
            for a, b, z in pairs_of
            for t in (2 * z, 2 * z + 1)
        ]
        return lax.ppermute(array, ("pp", "tp"), moves)

    micro = sections // 2
    entering = gathered_line(entry_stream_rows)
    entry = [between(entering, [(2 * k + u, 0, 2 * k) for k in range(micro)]) for u in range(2)]

    def groups(odd):
        lines = [((2 * i + 1) % sections, (2 * i + 2) % sections) if odd else (2 * i, 2 * i + 1) for i in range(micro)]
        return [
            [a * members + 2 * z, a * members + 2 * z + 1, b * members + 2 * z, b * members + 2 * z + 1]
            for a, b in lines
            for z in range(chips)
        ]

    def slot(index, odd, current, state):
        got = lax.all_gather(current, ("pp", "tp"), axis_index_groups=groups(odd))
        first = (index == layer).astype(jnp.int32)
        base = jnp.where(layer == 0, 2, 0) if odd else jnp.zeros((), jnp.int32)
        flags = jnp.stack([first, 1 - first, base.astype(jnp.int32), core.astype(jnp.int32)])
        return section(flags, got, gain, weights, edge, spike, out_gain, state)

    def two_slots(turn, carried):
        current, state = carried
        fresh = jnp.where(turn == 0, entry[0], entry[1])
        current = jnp.where(layer == 0, fresh, current)
        current, state = slot(2 * turn, True, current, state)
        return slot(2 * turn + 1, False, current, state)

    start = (jnp.zeros((SEG, half_width), jnp.bfloat16), jnp.zeros((pairs, 128, 128), jnp.float32))
    carried = lax.fori_loop(0, micro, two_slots, start)
    last = sections - 1
    finished = [between(carried[0], [(last, 2 * k, 2 * k) for k in range(micro)])]
    carried = two_slots(micro, carried)
    finished.append(between(carried[0], [(last, 2 * k + 1, 2 * k) for k in range(micro)]))
    mine = jnp.where(layer % 2 == 0, finished[0], finished[1])
    spread = mine.reshape(SEG, chips, HEAD).transpose(1, 0, 2)
    received = lax.all_to_all(spread, "tp", 0, 0, axis_index_groups=same_core)
    return lax.dynamic_index_in_dim(received, layer // 2 * 2, 0, keepdims=False)


def solution(mesh):
    in_specs = (
        P("pp", "tp"),
        P("pp", None),
        P("pp", "tp", None),
        P("pp", "tp", None),
        P("pp", "tp", None),
        P("pp", "tp", None),
        P("pp", "tp"),
        P("pp", None, "tp"),
        P("pp", None),
    )
    out_specs = P("pp", "tp")
    return jax.shard_map(shards, mesh=mesh, in_specs=in_specs, out_specs=out_specs, check_vma=False)
```

```python
import jax
import jax.numpy as jnp
from jax import lax
from jax.experimental import pallas as pl
from jax.experimental.pallas import tpu as pltpu
from jax.sharding import PartitionSpec as P

HEAD = 64
SEG = 64
EPSILON = 1e-06
NT = (((1,), (1,)), ((), ()))
NN = (((1,), (0,)), ((), ()))
TN = (((0,), (0,)), ((), ()))


def section_kernel(flags, got, gain, weights, edge, spike, out_gain, state_in, result, state, scaled, product):
    first, unit, base, core = flags[0], flags[1], flags[2], flags[3]
    rows, width = got.shape[1:]
    groups = weights.shape[0] // 4
    low = lax.broadcasted_iota(jnp.int32, (rows, 128), 1) < HEAD

    total = jnp.zeros((rows, 128), jnp.float32)
    for tile in range(width // 128):
        columns = pl.ds(tile * 128, 128)
        even = got[base, :, columns].astype(jnp.float32)
        odd = got[base + 1, :, columns].astype(jnp.float32)
        total = total + even * even + odd * odd
        left = jnp.where(low, even, pltpu.roll(odd, HEAD, 1))
        right = jnp.where(low, pltpu.roll(even, HEAD, 1), odd)
        for step, wide in enumerate((left, right)):
            columns = pl.ds((2 * tile + step) * 128, 128)
            scaled[:, columns] = (wide * gain[:, columns]).astype(jnp.bfloat16)
    total = jnp.sum(total, axis=1, keepdims=True)
    scale = jnp.broadcast_to(lax.rsqrt(total / (2 * width) + EPSILON), (rows, 128))

    at = lax.broadcasted_iota(jnp.int32, (rows, 2 * rows), 0)
    of = lax.broadcasted_iota(jnp.int32, (rows, 2 * rows), 1)
    ones = jnp.where(at >= jnp.where(of >= rows, of - rows, of), 1.0, 0.0).astype(jnp.bfloat16)
    at = lax.broadcasted_iota(jnp.int32, (2 * rows, rows), 0)
    of = lax.broadcasted_iota(jnp.int32, (2 * rows, rows), 1)
    causal = jnp.where(at >= rows, at - rows, at) >= of
    same = (lax.broadcasted_iota(jnp.int32, (128, 128), 0) < HEAD) == (
        lax.broadcasted_iota(jnp.int32, (128, 128), 1) < HEAD
    )
    mean = jnp.where(same, 1.0 / HEAD, 0.0).astype(jnp.bfloat16)
    mean = jnp.concatenate([mean, mean], axis=0)

    def halves(array):
        high = array.astype(jnp.bfloat16)
        return high, (array - high.astype(jnp.float32)).astype(jnp.bfloat16)

    def mix(pair, start):
        tiles = [product[:, start + 128 * k : start + 128 * k + 128] * scale for k in range(4)]
        rolled = [pltpu.roll(tile, HEAD, 1) for tile in tiles]
        query_pre = jnp.where(low, tiles[0], rolled[2])
        forget_pre = jnp.where(low, rolled[0], tiles[2])
        values = jnp.where(low, tiles[1], rolled[3]).astype(jnp.bfloat16)
        gate_pre = jnp.where(low, rolled[1], tiles[3])

        lower = edge[pair]
        upper = 1.0 - lower
        log_forget = jnp.log(lower + upper * jax.nn.sigmoid(forget_pre)) + spike[unit, pair]
        key_in = upper * jax.nn.sigmoid(-forget_pre)
        queries = query_pre * jax.nn.sigmoid(query_pre)
        running = lax.dot_general(
            ones, jnp.concatenate(halves(log_forget), axis=0), NN, preferred_element_type=jnp.float32
        )
        query_scaled = queries * jnp.exp(running)
        key_scaled = (key_in * jnp.exp(-running)).astype(jnp.bfloat16)
        stacked = jnp.concatenate(
            [jnp.where(low, query_scaled, 0.0), jnp.where(low, 0.0, query_scaled)], axis=0
        ).astype(jnp.bfloat16)
        scores = lax.dot_general(stacked, key_scaled, NT, preferred_element_type=jnp.float32)
        scores = jnp.where(causal, scores, 0.0).astype(jnp.bfloat16)
        both = lax.dot_general(scores, values, NN, preferred_element_type=jnp.float32)
        before = state[pair]
        mixed = jnp.where(low, both[:rows], both[rows:]) + lax.dot_general(
            query_scaled.astype(jnp.bfloat16),
            jnp.where(first == 1, 0.0, before).astype(jnp.bfloat16),
            NN,
            preferred_element_type=jnp.float32,
        )
        kept = (key_in * jnp.exp(running[rows - 1 :, :] - running)).astype(jnp.bfloat16)
        carried = lax.dot_general(kept, values, TN, preferred_element_type=jnp.float32)
        state[pair] = jnp.where(first == 1, jnp.where(same, carried, 0.0), before)
        average = lax.dot_general(
            jnp.concatenate(halves(mixed * mixed), axis=1), mean, NN, preferred_element_type=jnp.float32
        )
        branch = mixed * lax.rsqrt(average + EPSILON) * out_gain[...] * (gate_pre * jax.nn.sigmoid(gate_pre))
        columns = pl.ds(pl.multiple_of(pair * 128, 128), 128)
        own = got[base + core, :, columns].astype(jnp.float32)
        result[:, columns] = (own + branch).astype(jnp.bfloat16)

    def turn(index, _):
        now = jnp.maximum(index - 1, 0)
        mix(2 * now, 0)
        mix(2 * now + 1, 512)
        after = jnp.minimum(index, groups - 1)
        for head in range(4):
            product[:, 256 * head : 256 * head + 256] = lax.dot_general(
                scaled[...], weights[4 * after + head], NN, preferred_element_type=jnp.float32
            )
        return 0

    lax.fori_loop(0, groups + 1, turn, 0)


def hold_kernel(source, held, semaphores):
    copies = [
        pltpu.make_async_copy(source.at[head], held.at[head], semaphores.at[head]) for head in range(source.shape[0])
    ]
    for copy in copies:
        copy.start()
    for copy in copies:
        copy.wait()


def hold(weights):
    return pl.pallas_call(
        hold_kernel,
        out_shape=pltpu.VMEM(weights.shape, weights.dtype),
        in_specs=[pl.BlockSpec(memory_space=pltpu.HBM)],
        out_specs=pl.BlockSpec(memory_space=pltpu.VMEM),
        scratch_shapes=[pltpu.SemaphoreType.DMA((weights.shape[0],))],
        compiler_params=pltpu.CompilerParams(vmem_limit_bytes=1 << 20),
        cost_estimate=pl.CostEstimate(flops=0, bytes_accessed=4 * weights.size, transcendentals=0),
    )(weights)


def section(flags, got, gain, weights, edge, spike, out_gain, state):
    rows, width = got.shape[1:]
    return pl.pallas_call(
        section_kernel,
        out_shape=(
            jax.ShapeDtypeStruct((rows, width), jnp.bfloat16),
            jax.ShapeDtypeStruct(state.shape, state.dtype),
        ),
        in_specs=[pl.BlockSpec(memory_space=pltpu.SMEM)] + [pl.BlockSpec(memory_space=pltpu.VMEM)] * 7,
        out_specs=[pl.BlockSpec(memory_space=pltpu.VMEM)] * 2,
        scratch_shapes=[
            pltpu.VMEM((rows, 2 * width), jnp.bfloat16),
            pltpu.VMEM((rows, width), jnp.float32),
        ],
        input_output_aliases={7: 1},
        compiler_params=pltpu.CompilerParams(vmem_limit_bytes=24 << 20),
        cost_estimate=pl.CostEstimate(
            flops=2 * rows * weights.size, bytes_accessed=2 * weights.size, transcendentals=0
        ),
    )(flags, got, gain, weights, edge, spike, out_gain, state)


def shards(
    entry_stream_rows,
    layer_rescale_factor,
    probe_projection,
    retention_projection,
    candidate_projection,
    emission_filter_matrix,
    retention_minimum,
    decay_spike,
    per_group_scale,
):
    sections = lax.axis_size("pp")
    members = lax.axis_size("tp")
    chips = members // 2
    line = lax.axis_index("pp")
    across = 4
    turned = line // across % 2 == 1
    layer = jnp.where(turned, line + across - 1 - 2 * (line % across), line)
    place = [s + across - 1 - 2 * (s % across) if s // across % 2 else s for s in range(sections)]
    core = lax.axis_index("tp") % 2
    half_width = layer_rescale_factor.shape[1] // 2
    pairs = chips // 2
    same_core = [[c + 2 * z for z in range(chips)] for c in range(2)]

    def to_place(array):
        moved = lax.ppermute(array, "pp", [(s, place[s]) for s in range(sections) if place[s] != s])
        return jnp.where(turned, moved, array)

    local = jnp.stack(
        [probe_projection[0], retention_projection[0], candidate_projection[0], emission_filter_matrix[0]]
    )
    local = local.reshape(4 * HEAD, 2 * half_width).T
    weights = lax.all_gather(to_place(local), "tp", axis_index_groups=same_core)
    weights = hold(pltpu.with_memory_space_constraint(weights, pltpu.HBM))
    small = jnp.concatenate(
        [layer_rescale_factor[0], per_group_scale[0], retention_minimum[0], decay_spike[0, :, 0]]
    )
    small = to_place(small)
    gain = small[None, : 2 * half_width]
    out_gain = jnp.tile(small[None, 2 * half_width : 2 * half_width + HEAD], (1, 2))
    small = lax.all_gather(small[2 * half_width + HEAD :], "tp", axis_index_groups=same_core)
    edge = small[:, :HEAD].reshape(pairs, 1, 128)
    spike = small[:, HEAD:].reshape(pairs, 2, 2, SEG)
    spike = jnp.broadcast_to(spike.transpose(2, 0, 3, 1)[..., None], (2, pairs, SEG, 2, HEAD))
    spike = spike.reshape(2, pairs, SEG, 128)
    gain, out_gain, edge, spike = lax.optimization_barrier((gain, out_gain, edge, spike))

    def gathered_line(block):
        whole = lax.all_gather(block, "tp", axis_index_groups=same_core)
        return whole.transpose(1, 0, 2).reshape(block.shape[0], half_width)

    def between(array, pairs_of):
        moves = [
            (a * members + t, b * members + t)
            for a, b, z in pairs_of
            for t in (2 * z, 2 * z + 1)
        ]
        return lax.ppermute(array, ("pp", "tp"), moves)

    micro = sections // 2
    entering = gathered_line(entry_stream_rows)
    entry = [between(entering, [(2 * k + u, 0, 2 * k) for k in range(micro)]) for u in range(2)]

    def groups(odd):
        lines = [(2 * i + odd, (2 * i + 1 + odd) % sections) for i in range(micro)]
        lines = [(place[a], place[b]) for a, b in lines]
        return [
            [a * members + 2 * z, a * members + 2 * z + 1, b * members + 2 * z, b * members + 2 * z + 1]
            for a, b in lines
            for z in range(chips)
        ]

    def slot(index, odd, current, state):
        got = lax.all_gather(current, ("pp", "tp"), axis_index_groups=groups(odd))
        first = (index == layer).astype(jnp.int32)
        base = jnp.where(layer == 0, 2, 0) if odd else jnp.zeros((), jnp.int32)
        flags = jnp.stack([first, 1 - first, base.astype(jnp.int32), core.astype(jnp.int32)])
        return section(flags, got, gain, weights, edge, spike, out_gain, state)

    def two_slots(turn, carried):
        current, state = carried
        fresh = jnp.where(turn == 0, entry[0], entry[1])
        current = jnp.where(layer == 0, fresh, current)
        current, state = slot(2 * turn, True, current, state)
        return slot(2 * turn + 1, False, current, state)

    start = (jnp.zeros((SEG, half_width), jnp.bfloat16), jnp.zeros((pairs, 128, 128), jnp.float32))
    carried = start
    for turn in range(micro):
        carried = two_slots(turn, carried)
    last = place[sections - 1]
    finished = [between(carried[0], [(last, 2 * k, 2 * k) for k in range(micro)])]
    carried = two_slots(micro, carried)
    finished.append(between(carried[0], [(last, 2 * k + 1, 2 * k) for k in range(micro)]))
    mine = jnp.where(line % 2 == 0, finished[0], finished[1])
    spread = mine.reshape(SEG, chips, HEAD).transpose(1, 0, 2)
    received = lax.all_to_all(spread, "tp", 0, 0, axis_index_groups=same_core)
    return lax.dynamic_index_in_dim(received, line // 2 * 2, 0, keepdims=False)


def solution(mesh):
    in_specs = (
        P("pp", "tp"),
        P("pp", None),
        P("pp", "tp", None),
        P("pp", "tp", None),
        P("pp", "tp", None),
        P("pp", "tp", None),
        P("pp", "tp"),
        P("pp", None, "tp"),
        P("pp", None),
    )
    out_specs = P("pp", "tp")
    return jax.shard_map(shards, mesh=mesh, in_specs=in_specs, out_specs=out_specs, check_vma=False)
```

```python
import functools

import jax
import jax.numpy as jnp
from jax import lax
from jax.experimental import pallas as pl
from jax.experimental.pallas import tpu as pltpu
from jax.sharding import PartitionSpec as P

HEAD = 64
SEG = 64
EPSILON = 1e-06
NT = (((1,), (1,)), ((), ()))
NN = (((1,), (0,)), ((), ()))
TN = (((0,), (0,)), ((), ()))
ABREAST = 8


def section_kernel(
    slot,
    got,
    gain,
    weights,
    edge,
    spike,
    out_gain,
    state_in,
    keys_in,
    values_in,
    result,
    state,
    last_keys,
    last_values,
    scaled,
    product,
):
    line = lax.axis_index("pp")
    core = lax.axis_index("tp") % 2
    first = (line == slot).astype(jnp.int32)
    pairs = weights.shape[0] // 2

    @pl.when(line == slot - 1)
    def _():
        at = lax.broadcasted_iota(jnp.int32, (128, 128), 0) < HEAD
        of = lax.broadcasted_iota(jnp.int32, (128, 128), 1) < HEAD
        for pair in range(pairs):
            carried = lax.dot_general(last_keys[pair], last_values[pair], TN, preferred_element_type=jnp.float32)
            state[pair] = jnp.where(at == of, carried, 0.0)

    @pl.when((line == slot) | (line == slot - 2))
    def _():
        run_section(
            first, core, got, gain, weights, edge, spike, out_gain, result, state, last_keys, last_values, scaled, product
        )


def run_section(
    first, core, got, gain, weights, edge, spike, out_gain, result, state, last_keys, last_values, scaled, product
):
    rows, width = got.shape[1:]
    heads = weights.shape[0]
    low = lax.broadcasted_iota(jnp.int32, (rows, 128), 1) < HEAD

    total = jnp.zeros((rows, 128), jnp.float32)
    for tile in range(width // 128):
        columns = pl.ds(tile * 128, 128)
        even = got[0, :, columns].astype(jnp.float32)
        odd = got[1, :, columns].astype(jnp.float32)
        total = total + even * even + odd * odd
        left = jnp.where(low, even, pltpu.roll(odd, HEAD, 1))
        right = jnp.where(low, pltpu.roll(even, HEAD, 1), odd)
        for step, wide in enumerate((left, right)):
            columns = pl.ds((2 * tile + step) * 128, 128)
            scaled[:, columns] = (wide * gain[:, columns]).astype(jnp.bfloat16)
    total = jnp.sum(total, axis=1, keepdims=True)
    scale = jnp.broadcast_to(lax.rsqrt(total / (2 * width) + EPSILON), (rows, 128))

    at = lax.broadcasted_iota(jnp.int32, (rows, 2 * rows), 0)
    of = lax.broadcasted_iota(jnp.int32, (rows, 2 * rows), 1)
    ones = jnp.where(at >= jnp.where(of >= rows, of - rows, of), 1.0, 0.0).astype(jnp.bfloat16)
    at = lax.broadcasted_iota(jnp.int32, (2 * rows, rows), 0)
    of = lax.broadcasted_iota(jnp.int32, (2 * rows, rows), 1)
    causal = jnp.where(at >= rows, at - rows, at) >= of
    same = (lax.broadcasted_iota(jnp.int32, (128, 128), 0) < HEAD) == (
        lax.broadcasted_iota(jnp.int32, (128, 128), 1) < HEAD
    )
    mean = jnp.where(same, 1.0 / HEAD, 0.0).astype(jnp.bfloat16)

    def multiply(head, _):
        product[head] = lax.dot_general(scaled[...], weights[head], NN, preferred_element_type=jnp.float32)
        return 0

    lax.fori_loop(0, heads, multiply, 0, unroll=4)

    def several(index, _):
        pairs = [ABREAST * index + step for step in range(ABREAST)]
        queries, keys, forgets, values, gates = [], [], [], [], []
        for pair in pairs:
            tiles = [product[2 * pair + k // 2, :, 128 * (k % 2) : 128 * (k % 2) + 128] * scale for k in range(4)]
            rolled = [pltpu.roll(tile, HEAD, 1) for tile in tiles]
            query_pre = jnp.where(low, tiles[0], rolled[2])
            forget_pre = jnp.where(low, rolled[0], tiles[2])
            gate_pre = jnp.where(low, rolled[1], tiles[3])
            values.append(jnp.where(low, tiles[1], rolled[3]).astype(jnp.bfloat16))
            gates.append(gate_pre * jax.nn.sigmoid(gate_pre) * out_gain[...])
            queries.append(query_pre * jax.nn.sigmoid(query_pre))
            lower = edge[pair]
            upper = 1.0 - lower
            opposite = jnp.exp(jnp.minimum(-forget_pre, 80.0))
            kept = 1.0 / (1.0 + opposite)
            forgets.append(jnp.log(lower + upper * kept) + spike[1 - first, pair])
            keys.append(upper * (opposite * kept))

        running = []
        for step in range(0, ABREAST, 2):
            wide = jnp.concatenate(forgets[step : step + 2], axis=1)
            high = wide.astype(jnp.bfloat16)
            rest = (wide - high.astype(jnp.float32)).astype(jnp.bfloat16)
            wide = lax.dot_general(
                ones, jnp.concatenate([high, rest], axis=0), NN, preferred_element_type=jnp.float32
            )
            running += [wide[:, :128], wide[:, 128:]]

        squares, mixes = [], []
        for step, pair in enumerate(pairs):
            query_scaled = queries[step] * jnp.exp(running[step])
            key_scaled = (keys[step] * jnp.exp(-running[step])).astype(jnp.bfloat16)
            stacked = jnp.concatenate(
                [jnp.where(low, query_scaled, 0.0), jnp.where(low, 0.0, query_scaled)], axis=0
            ).astype(jnp.bfloat16)
            scores = lax.dot_general(stacked, key_scaled, NT, preferred_element_type=jnp.float32)
            scores = jnp.where(causal, scores, 0.0).astype(jnp.bfloat16)
            before = jnp.where(first == 1, 0.0, state[pair]).astype(jnp.bfloat16)
            both = lax.dot_general(
                jnp.concatenate([stacked, scores], axis=1),
                jnp.concatenate([before, values[step]], axis=0),
                NN,
                preferred_element_type=jnp.float32,
            )
            mixed = jnp.where(low, both[:rows], both[rows:])
            mixes.append(mixed)
            squares.append((mixed * mixed).astype(jnp.bfloat16))
            ending = running[step][rows - 1 :, :]
            last_keys[pair] = (keys[step] * jnp.exp(ending - running[step])).astype(jnp.bfloat16)
            last_values[pair] = values[step]

        average = lax.dot_general(
            jnp.concatenate(squares, axis=0), mean, NN, preferred_element_type=jnp.float32
        )
        for step, pair in enumerate(pairs):
            inverse = lax.rsqrt(average[rows * step : rows * step + rows] + EPSILON)
            columns = pl.ds(pl.multiple_of(pair * 128, 128), 128)
            own = got[core, :, columns].astype(jnp.float32)
            result[:, columns] = (own + mixes[step] * inverse * gates[step]).astype(jnp.bfloat16)
        return 0

    lax.fori_loop(0, heads // 2 // ABREAST, several, 0)


def hold_kernel(source, held, semaphores):
    copies = [
        pltpu.make_async_copy(source.at[head], held.at[head], semaphores.at[head]) for head in range(source.shape[0])
    ]
    for copy in copies:
        copy.start()
    for copy in copies:
        copy.wait()


def hold(weights):
    return pl.pallas_call(
        hold_kernel,
        out_shape=pltpu.VMEM(weights.shape, weights.dtype),
        in_specs=[pl.BlockSpec(memory_space=pltpu.HBM)],
        out_specs=pl.BlockSpec(memory_space=pltpu.VMEM),
        scratch_shapes=[pltpu.SemaphoreType.DMA((weights.shape[0],))],
        compiler_params=pltpu.CompilerParams(vmem_limit_bytes=1 << 20),
        cost_estimate=pl.CostEstimate(flops=0, bytes_accessed=4 * weights.size, transcendentals=0),
    )(weights)


def section(slot, got, gain, weights, edge, spike, out_gain, kept):
    rows, width = got.shape[1:]
    return pl.pallas_call(
        functools.partial(section_kernel, slot),
        out_shape=(
            jax.ShapeDtypeStruct((rows, width), jnp.bfloat16),
        )
        + tuple(jax.ShapeDtypeStruct(array.shape, array.dtype) for array in kept),
        in_specs=[pl.BlockSpec(memory_space=pltpu.VMEM)] * 9,
        out_specs=[pl.BlockSpec(memory_space=pltpu.VMEM)] * 4,
        scratch_shapes=[
            pltpu.VMEM((rows, 2 * width), jnp.bfloat16),
            pltpu.VMEM((weights.shape[0], rows, weights.shape[2]), jnp.float32),
        ],
        input_output_aliases={6: 1, 7: 2, 8: 3},
        compiler_params=pltpu.CompilerParams(vmem_limit_bytes=24 << 20),
        cost_estimate=pl.CostEstimate(
            flops=2 * rows * weights.size, bytes_accessed=2 * weights.size, transcendentals=0
        ),
    )(got, gain, weights, edge, spike, out_gain, *kept)


def shards(
    entry_stream_rows,
    layer_rescale_factor,
    probe_projection,
    retention_projection,
    candidate_projection,
    emission_filter_matrix,
    retention_minimum,
    decay_spike,
    per_group_scale,
):
    sections = lax.axis_size("pp")
    members = lax.axis_size("tp")
    chips = members // 2
    line = lax.axis_index("pp")
    half_width = layer_rescale_factor.shape[1] // 2
    pairs = chips // 2
    same_core = [[c + 2 * z for z in range(chips)] for c in range(2)]

    local = jnp.stack(
        [probe_projection[0], retention_projection[0], candidate_projection[0], emission_filter_matrix[0]]
    )
    local = local.reshape(4 * HEAD, 2 * half_width).T
    weights = lax.all_gather(local, "tp", axis_index_groups=same_core)
    weights = hold(pltpu.with_memory_space_constraint(weights, pltpu.HBM))
    small = jnp.concatenate(
        [layer_rescale_factor[0], per_group_scale[0], retention_minimum[0], decay_spike[0, :, 0]]
    )
    gain = small[None, : 2 * half_width]
    out_gain = jnp.tile(small[None, 2 * half_width : 2 * half_width + HEAD], (1, 2))
    small = lax.all_gather(small[2 * half_width + HEAD :], "tp", axis_index_groups=same_core)
    edge = small[:, :HEAD].reshape(pairs, 1, 128)
    spike = small[:, HEAD:].reshape(pairs, 2, 2, SEG)
    spike = jnp.broadcast_to(spike.transpose(2, 0, 3, 1)[..., None], (2, pairs, SEG, 2, HEAD))
    spike = spike.reshape(2, pairs, SEG, 128)
    gain, out_gain, edge, spike = lax.optimization_barrier((gain, out_gain, edge, spike))

    def gathered_line(block):
        whole = lax.all_gather(block, "tp", axis_index_groups=same_core)
        return whole.transpose(1, 0, 2).reshape(block.shape[0], half_width)

    def between(array, pairs_of):
        moves = [
            (a * members + t, b * members + t)
            for a, b, z in pairs_of
            for t in (2 * z, 2 * z + 1)
        ]
        return lax.ppermute(array, ("pp", "tp"), moves)

    micro = sections // 2
    entering = gathered_line(entry_stream_rows)
    entry = [between(entering, [(2 * k + u, 0, 2 * k) for k in range(micro)]) for u in range(2)]

    def groups(slot):
        paired, found = set(), []
        for unit in range(2):
            a, b = slot - 2 * unit - 1, slot - 2 * unit
            if a >= 0 and b < sections:
                paired |= {a, b}
                found += [[l * members + 2 * z + c for l in (a, b) for c in range(2)] for z in range(chips)]
        for l in range(sections):
            if l not in paired:
                found += [[l * members + 4 * z + t for t in range(4)] for z in range(pairs)]
        return found

    current = jnp.zeros((SEG, half_width), jnp.bfloat16)
    kept = (jnp.zeros((pairs, 128, 128), jnp.float32),) + (jnp.zeros((pairs, SEG, 128), jnp.bfloat16),) * 2
    finished = []
    for slot in range(sections + 2):
        if slot in (0, 2):
            current = jnp.where(line == 0, entry[slot // 2], current)
        got = lax.all_gather(current, ("pp", "tp"), axis_index_groups=groups(slot))
        current, *kept = section(slot, got, gain, weights, edge, spike, out_gain, kept)
        if slot in (sections - 1, sections + 1):
            unit = len(finished)
            finished.append(between(current, [(sections - 1, 2 * k + unit, 2 * k) for k in range(micro)]))
    mine = jnp.where(line % 2 == 0, finished[0], finished[1])
    spread = mine.reshape(SEG, chips, HEAD).transpose(1, 0, 2)
    received = lax.all_to_all(spread, "tp", 0, 0, axis_index_groups=same_core)
    return lax.dynamic_index_in_dim(received, line // 2 * 2, 0, keepdims=False)


def solution(mesh):
    in_specs = (
        P("pp", "tp"),
        P("pp", None),
        P("pp", "tp", None),
        P("pp", "tp", None),
        P("pp", "tp", None),
        P("pp", "tp", None),
        P("pp", "tp"),
        P("pp", None, "tp"),
        P("pp", None),
    )
    out_specs = P("pp", "tp")
    return jax.shard_map(shards, mesh=mesh, in_specs=in_specs, out_specs=out_specs, check_vma=False)
```

```python
import functools

import jax
import jax.numpy as jnp
from jax import lax
from jax.experimental import pallas as pl
from jax.experimental.pallas import tpu as pltpu
from jax.sharding import PartitionSpec as P

HEAD = 64
SEG = 64
EPSILON = 1e-06
NT = (((1,), (1,)), ((), ()))
NN = (((1,), (0,)), ((), ()))
TN = (((0,), (0,)), ((), ()))
ABREAST = 8


def section_kernel(
    slot,
    got,
    gain,
    weights,
    edge,
    spike,
    out_gain,
    state_in,
    keys_in,
    values_in,
    result,
    weights_out,
    state,
    last_keys,
    last_values,
    scaled,
    product,
):
    line = lax.axis_index("pp")
    core = lax.axis_index("tp") % 2
    first = (line == slot).astype(jnp.int32)
    pairs = weights.shape[0] // 2

    @pl.when(line == slot - 1)
    def _():
        at = lax.broadcasted_iota(jnp.int32, (128, 128), 0) < HEAD
        of = lax.broadcasted_iota(jnp.int32, (128, 128), 1) < HEAD
        for pair in range(pairs):
            carried = lax.dot_general(last_keys[pair], last_values[pair], TN, preferred_element_type=jnp.float32)
            state[pair] = jnp.where(at == of, carried, 0.0)

    @pl.when((line == slot) | (line == slot - 2))
    def _():
        run_section(
            first, core, got, gain, weights, edge, spike, out_gain, result, state, last_keys, last_values, scaled, product
        )


def run_section(
    first, core, got, gain, weights, edge, spike, out_gain, result, state, last_keys, last_values, scaled, product
):
    rows, width = got.shape[1:]
    heads = weights.shape[0]
    low = lax.broadcasted_iota(jnp.int32, (rows, 128), 1) < HEAD

    total = jnp.zeros((rows, 128), jnp.float32)
    for tile in range(width // 128):
        columns = pl.ds(tile * 128, 128)
        even = got[0, :, columns].astype(jnp.float32)
        odd = got[1, :, columns].astype(jnp.float32)
        total = total + even * even + odd * odd
        left = jnp.where(low, even, pltpu.roll(odd, HEAD, 1))
        right = jnp.where(low, pltpu.roll(even, HEAD, 1), odd)
        for step, wide in enumerate((left, right)):
            columns = pl.ds((2 * tile + step) * 128, 128)
            scaled[:, columns] = (wide * gain[:, columns]).astype(jnp.bfloat16)
    total = jnp.sum(total, axis=1, keepdims=True)
    scale = jnp.broadcast_to(lax.rsqrt(total / (2 * width) + EPSILON), (rows, 128))

    at = lax.broadcasted_iota(jnp.int32, (rows, 2 * rows), 0)
    of = lax.broadcasted_iota(jnp.int32, (rows, 2 * rows), 1)
    ones = jnp.where(at >= jnp.where(of >= rows, of - rows, of), 1.0, 0.0).astype(jnp.bfloat16)
    at = lax.broadcasted_iota(jnp.int32, (2 * rows, rows), 0)
    of = lax.broadcasted_iota(jnp.int32, (2 * rows, rows), 1)
    causal = jnp.where(at >= rows, at - rows, at) >= of
    same = (lax.broadcasted_iota(jnp.int32, (128, 128), 0) < HEAD) == (
        lax.broadcasted_iota(jnp.int32, (128, 128), 1) < HEAD
    )
    mean = jnp.where(same, 1.0 / HEAD, 0.0).astype(jnp.bfloat16)

    def multiply(head, _):
        product[head] = lax.dot_general(scaled[...], weights[head], NN, preferred_element_type=jnp.float32)
        return 0

    lax.fori_loop(0, heads, multiply, 0, unroll=4)

    def several(index, _):
        pairs = [ABREAST * index + step for step in range(ABREAST)]
        queries, keys, forgets, values, gates = [], [], [], [], []
        for pair in pairs:
            tiles = [product[2 * pair + k // 2, :, 128 * (k % 2) : 128 * (k % 2) + 128] * scale for k in range(4)]
            rolled = [pltpu.roll(tile, HEAD, 1) for tile in tiles]
            query_pre = jnp.where(low, tiles[0], rolled[2])
            forget_pre = jnp.where(low, rolled[0], tiles[2])
            gate_pre = jnp.where(low, rolled[1], tiles[3])
            values.append(jnp.where(low, tiles[1], rolled[3]).astype(jnp.bfloat16))
            gates.append(gate_pre * jax.nn.sigmoid(gate_pre) * out_gain[...])
            queries.append(query_pre * jax.nn.sigmoid(query_pre))
            lower = edge[pair]
            upper = 1.0 - lower
            opposite = jnp.exp(jnp.minimum(-forget_pre, 80.0))
            kept = 1.0 / (1.0 + opposite)
            forgets.append(jnp.log(lower + upper * kept) + spike[1 - first, pair])
            keys.append(upper * (opposite * kept))

        running = []
        for step in range(0, ABREAST, 2):
            wide = jnp.concatenate(forgets[step : step + 2], axis=1)
            high = wide.astype(jnp.bfloat16)
            rest = (wide - high.astype(jnp.float32)).astype(jnp.bfloat16)
            wide = lax.dot_general(
                ones, jnp.concatenate([high, rest], axis=0), NN, preferred_element_type=jnp.float32
            )
            running += [wide[:, :128], wide[:, 128:]]

        squares, mixes = [], []
        for step, pair in enumerate(pairs):
            query_scaled = queries[step] * jnp.exp(running[step])
            key_scaled = (keys[step] * jnp.exp(-running[step])).astype(jnp.bfloat16)
            stacked = jnp.concatenate(
                [jnp.where(low, query_scaled, 0.0), jnp.where(low, 0.0, query_scaled)], axis=0
            ).astype(jnp.bfloat16)
            scores = lax.dot_general(stacked, key_scaled, NT, preferred_element_type=jnp.float32)
            scores = jnp.where(causal, scores, 0.0).astype(jnp.bfloat16)
            before = jnp.where(first == 1, 0.0, state[pair]).astype(jnp.bfloat16)
            both = lax.dot_general(
                jnp.concatenate([stacked, scores], axis=1),
                jnp.concatenate([before, values[step]], axis=0),
                NN,
                preferred_element_type=jnp.float32,
            )
            mixed = jnp.where(low, both[:rows], both[rows:])
            mixes.append(mixed)
            squares.append((mixed * mixed).astype(jnp.bfloat16))
            ending = running[step][rows - 1 :, :]
            last_keys[pair] = (keys[step] * jnp.exp(ending - running[step])).astype(jnp.bfloat16)
            last_values[pair] = values[step]

        average = lax.dot_general(
            jnp.concatenate(squares, axis=0), mean, NN, preferred_element_type=jnp.float32
        )
        for step, pair in enumerate(pairs):
            inverse = lax.rsqrt(average[rows * step : rows * step + rows] + EPSILON)
            columns = pl.ds(pl.multiple_of(pair * 128, 128), 128)
            own = got[core, :, columns].astype(jnp.float32)
            result[:, columns] = (own + mixes[step] * inverse * gates[step]).astype(jnp.bfloat16)
        return 0

    lax.fori_loop(0, heads // 2 // ABREAST, several, 0)


def hold_kernel(skipped, count, plan, *refs):
    sources, target, semaphores = refs[skipped : skipped + count], refs[skipped + count], refs[-1]
    row = lax.axis_index("pp") // 4
    for rows, moves in plan:
        wanted = row == rows[0]
        for other in rows[1:]:
            wanted = wanted | (row == other)

        @pl.when(wanted)
        def _():
            copies = []
            for index, quarter in moves:
                source = sources[index]
                depth = source.shape[1]
                for head in range(source.shape[0]):
                    copies.append(
                        pltpu.make_async_copy(
                            source.at[head],
                            target.at[head, pl.ds(quarter * depth, depth)],
                            semaphores.at[quarter * source.shape[0] + head],
                        )
                    )
            for copy in copies:
                copy.start()
            for copy in copies:
                copy.wait()


def hold(plan, sources, before=None, after=None, along=None):
    heads, depth, columns = sources[0].shape
    sources = [pltpu.with_memory_space_constraint(source, pltpu.HBM) for source in sources]
    extra = [array for array in (before, after, along) if array is not None]
    held = pltpu.VMEM((heads, 4 * depth, columns), sources[0].dtype)
    outputs = (held,) if along is None else (held, jax.ShapeDtypeStruct(along.shape, along.dtype))
    aliases = {} if before is None else {0: 0}
    if along is not None:
        aliases[len(extra) - 1] = 1
    results = pl.pallas_call(
        functools.partial(hold_kernel, len(extra), len(sources), plan),
        out_shape=outputs,
        in_specs=[pl.BlockSpec(memory_space=pltpu.VMEM)] * len(extra)
        + [pl.BlockSpec(memory_space=pltpu.HBM)] * len(sources),
        out_specs=[pl.BlockSpec(memory_space=pltpu.VMEM)] * len(outputs),
        scratch_shapes=[pltpu.SemaphoreType.DMA((4 * heads,))],
        input_output_aliases=aliases,
        compiler_params=pltpu.CompilerParams(vmem_limit_bytes=24 << 20),
        cost_estimate=pl.CostEstimate(
            flops=0, bytes_accessed=4 * len(sources) * sources[0].size, transcendentals=0
        ),
    )(*extra, *sources)
    return results[0] if along is None else results


def gate_kernel(*refs):
    pass


def gate(array, after):
    return pl.pallas_call(
        gate_kernel,
        out_shape=pltpu.HBM(array.shape, array.dtype),
        in_specs=[pl.BlockSpec(memory_space=pltpu.HBM), pl.BlockSpec(memory_space=pl.ANY)],
        out_specs=pl.BlockSpec(memory_space=pltpu.HBM),
        input_output_aliases={0: 0},
        compiler_params=pltpu.CompilerParams(vmem_limit_bytes=1 << 20),
    )(pltpu.with_memory_space_constraint(array, pltpu.HBM), after)


def section(slot, got, gain, weights, edge, spike, out_gain, kept):
    rows, width = got.shape[1:]
    return pl.pallas_call(
        functools.partial(section_kernel, slot),
        out_shape=(
            jax.ShapeDtypeStruct((rows, width), jnp.bfloat16),
            pltpu.VMEM(weights.shape, weights.dtype),
        )
        + tuple(jax.ShapeDtypeStruct(array.shape, array.dtype) for array in kept),
        in_specs=[pl.BlockSpec(memory_space=pltpu.VMEM)] * 9,
        out_specs=[pl.BlockSpec(memory_space=pltpu.VMEM)] * 5,
        scratch_shapes=[
            pltpu.VMEM((rows, 2 * width), jnp.bfloat16),
            pltpu.VMEM((weights.shape[0], rows, weights.shape[2]), jnp.float32),
        ],
        input_output_aliases={2: 1, 6: 2, 7: 3, 8: 4},
        compiler_params=pltpu.CompilerParams(vmem_limit_bytes=24 << 20),
        cost_estimate=pl.CostEstimate(
            flops=2 * rows * weights.size, bytes_accessed=2 * weights.size, transcendentals=0
        ),
    )(got, gain, weights, edge, spike, out_gain, *kept)


def shards(
    entry_stream_rows,
    layer_rescale_factor,
    probe_projection,
    retention_projection,
    candidate_projection,
    emission_filter_matrix,
    retention_minimum,
    decay_spike,
    per_group_scale,
):
    sections = lax.axis_size("pp")
    members = lax.axis_size("tp")
    chips = members // 2
    line = lax.axis_index("pp")
    half_width = layer_rescale_factor.shape[1] // 2
    pairs = chips // 2
    same_core = [[c + 2 * z for z in range(chips)] for c in range(2)]

    local = jnp.stack(
        [probe_projection[0], retention_projection[0], candidate_projection[0], emission_filter_matrix[0]]
    )
    local = local.reshape(4 * HEAD, 2 * half_width).T
    quarters = jnp.split(local, 4)
    row = line // 4
    last = sections // 4 - 1
    down = [(x * members + t, (last * 4 + x) * members + t) for x in range(4) for t in range(members)]
    up = [(b, a) for a, b in down]
    swapped = lax.ppermute(quarters[3], ("pp", "tp"), down + up)
    same_lines = [[l * members + t for t in same_core[c]] for l in range(sections) for c in range(2)]
    blocks = []
    for index in range(4):
        ours = jnp.where(row == last, swapped if index == 0 else quarters[index - 1], quarters[index])
        if index == 3:
            started = pltpu.with_memory_space_constraint(blocks[0], pltpu.HBM)
            ours = gate(jnp.where(row == 0, swapped, ours), started)
        turned = same_lines[index:] + same_lines[:index]
        blocks.append(lax.all_gather(ours, ("pp", "tp"), axis_index_groups=turned))
    up = [(b, a) for b, a in up if a % members % 4 < 2]
    down = [(a, b) for a, b in down if a % members % 4 < 2]
    returned = lax.ppermute(blocks[0], ("pp", "tp"), up)
    whole_plan = list(enumerate(range(4)))
    weights = hold([((0,), whole_plan)], blocks[:3] + [returned])
    gain = layer_rescale_factor
    out_gain = jnp.tile(per_group_scale, (1, 2))
    rest = jnp.concatenate([retention_minimum[0], decay_spike[0, :, 0]])
    parts = []
    for _ in range(3):
        part = lax.reduce_precision(rest, 8, 7)
        parts.append(part.astype(jnp.bfloat16))
        rest = rest - part
    parts = jnp.concatenate(parts).reshape(-1, HEAD)
    extra = parts.shape[0]
    padding = jnp.zeros((16 - extra, HEAD), jnp.bfloat16)
    whole = lax.all_gather(
        jnp.concatenate([entry_stream_rows, parts, padding]), "tp", axis_index_groups=same_core
    )
    entering = whole[:, :SEG].transpose(1, 0, 2).reshape(SEG, half_width)
    small = whole[:, SEG : SEG + extra].astype(jnp.float32).reshape(chips, 3, 3 * HEAD).sum(axis=1)
    edge = small[:, :HEAD].reshape(pairs, 1, 128)
    spike = small[:, HEAD:].reshape(pairs, 2, 2, SEG)
    spike = jnp.broadcast_to(spike.transpose(2, 0, 3, 1)[..., None], (2, pairs, SEG, 2, HEAD))
    spike = spike.reshape(2, pairs, SEG, 128)
    gain, out_gain, edge, spike = lax.optimization_barrier((gain, out_gain, edge, spike))

    def between(array, pairs_of):
        moves = [
            (a * members + t, b * members + t)
            for a, b, z in pairs_of
            for t in (2 * z, 2 * z + 1)
        ]
        return lax.ppermute(array, ("pp", "tp"), moves)

    micro = sections // 2
    entry = [between(entering, [(2 * k + u, 0, 2 * k) for k in range(micro)]) for u in range(2)]

    def groups(slot):
        paired, found = set(), []
        for unit in range(2):
            a, b = slot - 2 * unit - 1, slot - 2 * unit
            if a >= 0 and b < sections:
                paired |= {a, b}
                found += [[l * members + 2 * z + c for l in (a, b) for c in range(2)] for z in range(chips)]
        for l in range(sections):
            if l not in paired:
                found += [[l * members + 4 * z + t for t in range(4)] for z in range(pairs)]
        return found

    current = jnp.zeros((SEG, half_width), jnp.bfloat16)
    kept = (jnp.zeros((pairs, 128, 128), jnp.float32),) + (jnp.zeros((pairs, SEG, 128), jnp.bfloat16),) * 2
    finished = []
    for slot in range(sections + 2):
        if slot in (0, 2):
            current = jnp.where(line == 0, entry[slot // 2], current)
        if slot == 4:
            blocks[3] = gate(blocks[3], current)
            weights, current = hold(
                [((1, 2), whole_plan), ((3,), [(1, 0), (2, 1), (3, 2)])], blocks, along=current
            )
            sent = lax.ppermute(blocks[3], ("pp", "tp"), down)
        if slot == 12:
            weights = hold([((3,), [(0, 3)])], [sent], before=weights)
        got = lax.all_gather(current, ("pp", "tp"), axis_index_groups=groups(slot))
        if slot == 4:
            weights = hold([((0,), whole_plan)], blocks[:3] + [returned], before=weights, after=got)
        current, weights, *kept = section(slot, got, gain, weights, edge, spike, out_gain, kept)
        if slot in (sections - 1, sections + 1):
            unit = len(finished)
            finished.append(between(current, [(sections - 1, 2 * k + unit, 2 * k) for k in range(micro)]))
    mine = jnp.where(line % 2 == 0, finished[0], finished[1])
    spread = mine.reshape(SEG, chips, HEAD).transpose(1, 0, 2)
    received = lax.all_to_all(spread, "tp", 0, 0, axis_index_groups=same_core)
    return lax.dynamic_index_in_dim(received, line // 2 * 2, 0, keepdims=False)


def solution(mesh):
    in_specs = (
        P("pp", "tp"),
        P("pp", None),
        P("pp", "tp", None),
        P("pp", "tp", None),
        P("pp", "tp", None),
        P("pp", "tp", None),
        P("pp", "tp"),
        P("pp", None, "tp"),
        P("pp", None),
    )
    out_specs = P("pp", "tp")
    return jax.shard_map(shards, mesh=mesh, in_specs=in_specs, out_specs=out_specs, check_vma=False)
```

```python
import functools

import jax
import jax.numpy as jnp
from jax import lax
from jax.experimental import pallas as pl
from jax.experimental.pallas import tpu as pltpu
from jax.sharding import PartitionSpec as P

HEAD = 64
SEG = 64
EPSILON = 1e-06
NT = (((1,), (1,)), ((), ()))
NN = (((1,), (0,)), ((), ()))
TN = (((0,), (0,)), ((), ()))
ABREAST = 8


def section_kernel(
    slot,
    got,
    gain,
    weights,
    edge,
    spike,
    out_gain,
    state_in,
    keys_in,
    values_in,
    *others,
):
    result, state, last_keys, last_values, scaled, product = others[-6:]
    line = lax.axis_index("pp")
    core = lax.axis_index("tp") % 2
    first = (line == slot).astype(jnp.int32)
    pairs = weights.shape[0] // 2

    @pl.when(line == slot - 1)
    def _():
        at = lax.broadcasted_iota(jnp.int32, (128, 128), 0) < HEAD
        of = lax.broadcasted_iota(jnp.int32, (128, 128), 1) < HEAD
        for pair in range(pairs):
            carried = lax.dot_general(last_keys[pair], last_values[pair], TN, preferred_element_type=jnp.float32)
            state[pair] = jnp.where(at == of, carried, 0.0)

    @pl.when((line == slot) | (line == slot - 2))
    def _():
        run_section(
            first, core, got, gain, weights, edge, spike, out_gain, result, state, last_keys, last_values, scaled, product
        )


def run_section(
    first, core, got, gain, weights, edge, spike, out_gain, result, state, last_keys, last_values, scaled, product
):
    rows, width = got.shape[1:]
    heads = weights.shape[0]
    low = lax.broadcasted_iota(jnp.int32, (rows, 128), 1) < HEAD

    total = jnp.zeros((rows, 128), jnp.float32)
    for tile in range(width // 128):
        columns = pl.ds(tile * 128, 128)
        even = got[0, :, columns].astype(jnp.float32)
        odd = got[1, :, columns].astype(jnp.float32)
        total = total + even * even + odd * odd
        left = jnp.where(low, even, pltpu.roll(odd, HEAD, 1))
        right = jnp.where(low, pltpu.roll(even, HEAD, 1), odd)
        for step, wide in enumerate((left, right)):
            columns = pl.ds((2 * tile + step) * 128, 128)
            scaled[:, columns] = (wide * gain[:, columns]).astype(jnp.bfloat16)
    total = jnp.sum(total, axis=1, keepdims=True)
    scale = jnp.broadcast_to(lax.rsqrt(total / (2 * width) + EPSILON), (rows, 128))

    at = lax.broadcasted_iota(jnp.int32, (rows, 2 * rows), 0)
    of = lax.broadcasted_iota(jnp.int32, (rows, 2 * rows), 1)
    ones = jnp.where(at >= jnp.where(of >= rows, of - rows, of), 1.0, 0.0).astype(jnp.bfloat16)
    at = lax.broadcasted_iota(jnp.int32, (2 * rows, rows), 0)
    of = lax.broadcasted_iota(jnp.int32, (2 * rows, rows), 1)
    causal = jnp.where(at >= rows, at - rows, at) >= of
    same = (lax.broadcasted_iota(jnp.int32, (128, 128), 0) < HEAD) == (
        lax.broadcasted_iota(jnp.int32, (128, 128), 1) < HEAD
    )
    mean = jnp.where(same, 1.0 / HEAD, 0.0).astype(jnp.bfloat16)

    def multiply(head, _):
        product[head] = lax.dot_general(scaled[...], weights[head], NN, preferred_element_type=jnp.float32)
        return 0

    lax.fori_loop(0, heads, multiply, 0, unroll=8)

    def several(index, _):
        pairs = [ABREAST * index + step for step in range(ABREAST)]
        queries, keys, forgets, values, gates = [], [], [], [], []
        for pair in pairs:
            tiles = [product[2 * pair + k // 2, :, 128 * (k % 2) : 128 * (k % 2) + 128] * scale for k in range(4)]
            rolled = [pltpu.roll(tile, HEAD, 1) for tile in tiles]
            query_pre = jnp.where(low, tiles[0], rolled[2])
            forget_pre = jnp.where(low, rolled[0], tiles[2])
            gate_pre = jnp.where(low, rolled[1], tiles[3])
            values.append(jnp.where(low, tiles[1], rolled[3]).astype(jnp.bfloat16))
            gates.append(gate_pre * jax.nn.sigmoid(gate_pre) * out_gain[...])
            queries.append(query_pre * jax.nn.sigmoid(query_pre))
            lower = edge[pair]
            upper = 1.0 - lower
            opposite = jnp.exp(jnp.minimum(-forget_pre, 80.0))
            kept = 1.0 / (1.0 + opposite)
            forgets.append(jnp.log(lower + upper * kept) + spike[1 - first, pair])
            keys.append(upper * (opposite * kept))

        running = []
        for step in range(0, ABREAST, 2):
            wide = jnp.concatenate(forgets[step : step + 2], axis=1)
            high = wide.astype(jnp.bfloat16)
            rest = (wide - high.astype(jnp.float32)).astype(jnp.bfloat16)
            wide = lax.dot_general(
                ones, jnp.concatenate([high, rest], axis=0), NN, preferred_element_type=jnp.float32
            )
            running += [wide[:, :128], wide[:, 128:]]

        squares, mixes = [], []
        for step, pair in enumerate(pairs):
            query_scaled = queries[step] * jnp.exp(running[step])
            key_scaled = (keys[step] * jnp.exp(-running[step])).astype(jnp.bfloat16)
            stacked = jnp.concatenate(
                [jnp.where(low, query_scaled, 0.0), jnp.where(low, 0.0, query_scaled)], axis=0
            ).astype(jnp.bfloat16)
            scores = lax.dot_general(stacked, key_scaled, NT, preferred_element_type=jnp.float32)
            scores = jnp.where(causal, scores, 0.0).astype(jnp.bfloat16)
            before = jnp.where(first == 1, 0.0, state[pair]).astype(jnp.bfloat16)
            both = lax.dot_general(
                jnp.concatenate([stacked, scores], axis=1),
                jnp.concatenate([before, values[step]], axis=0),
                NN,
                preferred_element_type=jnp.float32,
            )
            mixed = jnp.where(low, both[:rows], both[rows:])
            mixes.append(mixed)
            squares.append((mixed * mixed).astype(jnp.bfloat16))
            ending = running[step][rows - 1 :, :]
            last_keys[pair] = (keys[step] * jnp.exp(ending - running[step])).astype(jnp.bfloat16)
            last_values[pair] = values[step]

        average = lax.dot_general(
            jnp.concatenate(squares, axis=0), mean, NN, preferred_element_type=jnp.float32
        )
        for step, pair in enumerate(pairs):
            inverse = lax.rsqrt(average[rows * step : rows * step + rows] + EPSILON)
            columns = pl.ds(pl.multiple_of(pair * 128, 128), 128)
            own = got[core, :, columns].astype(jnp.float32)
            result[:, columns] = (own + mixes[step] * inverse * gates[step]).astype(jnp.bfloat16)
        return 0

    lax.fori_loop(0, heads // 2 // ABREAST, several, 0)


def hold_kernel(source, held, semaphores):
    copies = [
        pltpu.make_async_copy(source.at[head], held.at[head], semaphores.at[head]) for head in range(source.shape[0])
    ]
    for copy in copies:
        copy.start()
    for copy in copies:
        copy.wait()


def hold(weights):
    return pl.pallas_call(
        hold_kernel,
        out_shape=pltpu.VMEM(weights.shape, weights.dtype),
        in_specs=[pl.BlockSpec(memory_space=pltpu.HBM)],
        out_specs=pl.BlockSpec(memory_space=pltpu.VMEM),
        scratch_shapes=[pltpu.SemaphoreType.DMA((weights.shape[0],))],
        compiler_params=pltpu.CompilerParams(vmem_limit_bytes=1 << 20),
        cost_estimate=pl.CostEstimate(flops=0, bytes_accessed=4 * weights.size, transcendentals=0),
    )(weights)


def section(slot, got, gain, weights, edge, spike, out_gain, kept, after):
    rows, width = got.shape[1:]
    return pl.pallas_call(
        functools.partial(section_kernel, slot),
        out_shape=(
            jax.ShapeDtypeStruct((rows, width), jnp.bfloat16),
        )
        + tuple(jax.ShapeDtypeStruct(array.shape, array.dtype) for array in kept),
        in_specs=[pl.BlockSpec(memory_space=pltpu.VMEM)] * (9 + len(after)),
        out_specs=[pl.BlockSpec(memory_space=pltpu.VMEM)] * 4,
        scratch_shapes=[
            pltpu.VMEM((rows, 2 * width), jnp.bfloat16),
            pltpu.VMEM((weights.shape[0], rows, weights.shape[2]), jnp.float32),
        ],
        input_output_aliases={6: 1, 7: 2, 8: 3},
        compiler_params=pltpu.CompilerParams(vmem_limit_bytes=24 << 20),
        cost_estimate=pl.CostEstimate(
            flops=2 * rows * weights.size, bytes_accessed=2 * weights.size, transcendentals=0
        ),
    )(got, gain, weights, edge, spike, out_gain, *kept, *after)


def shards(
    entry_stream_rows,
    layer_rescale_factor,
    probe_projection,
    retention_projection,
    candidate_projection,
    emission_filter_matrix,
    retention_minimum,
    decay_spike,
    per_group_scale,
):
    sections = lax.axis_size("pp")
    members = lax.axis_size("tp")
    chips = members // 2
    line = lax.axis_index("pp")
    half_width = layer_rescale_factor.shape[1] // 2
    pairs = chips // 2
    same_core = [[c + 2 * z for z in range(chips)] for c in range(2)]

    local = jnp.stack(
        [probe_projection[0], retention_projection[0], candidate_projection[0], emission_filter_matrix[0]]
    )
    local = local.reshape(4 * HEAD, 2 * half_width).T
    weights = lax.all_gather(local, "tp", axis_index_groups=same_core)
    weights = hold(pltpu.with_memory_space_constraint(weights, pltpu.HBM))
    gain = layer_rescale_factor
    out_gain = jnp.tile(per_group_scale, (1, 2))
    rest = jnp.concatenate([retention_minimum[0], decay_spike[0, :, 0]])
    parts = []
    for _ in range(3):
        part = lax.reduce_precision(rest, 8, 7)
        parts.append(part.astype(jnp.bfloat16))
        rest = rest - part
    parts = jnp.concatenate(parts).reshape(-1, HEAD)
    extra = parts.shape[0]
    padding = jnp.zeros((16 - extra, HEAD), jnp.bfloat16)
    whole = lax.all_gather(
        jnp.concatenate([entry_stream_rows, parts, padding]), "tp", axis_index_groups=same_core
    )
    entering = whole[:, :SEG].transpose(1, 0, 2).reshape(SEG, half_width)
    small = whole[:, SEG : SEG + extra].astype(jnp.float32).reshape(chips, 3, 3 * HEAD).sum(axis=1)
    edge = small[:, :HEAD].reshape(pairs, 1, 128)
    spike = small[:, HEAD:].reshape(pairs, 2, 2, SEG)
    spike = jnp.broadcast_to(spike.transpose(2, 0, 3, 1)[..., None], (2, pairs, SEG, 2, HEAD))
    spike = spike.reshape(2, pairs, SEG, 128)
    gain, out_gain, edge, spike = lax.optimization_barrier((gain, out_gain, edge, spike))

    def between(array, pairs_of):
        moves = [
            (a * members + 2 * z + c, b * members + 2 * y + c) for a, b, z, y in pairs_of for c in range(2)
        ]
        return lax.ppermute(array, ("pp", "tp"), moves)

    micro = sections // 2
    entry = [between(entering, [(2 * k + u, 0, 2 * k, 2 * k) for k in range(micro)]) for u in range(2)]

    def groups(slot):
        paired, found = set(), []
        for unit in range(2):
            a, b = slot - 2 * unit - 1, slot - 2 * unit
            if a >= 0 and b < sections:
                paired |= {a, b}
                found += [[l * members + 2 * z + c for l in (a, b) for c in range(2)] for z in range(chips)]
        for l in range(sections):
            if l not in paired:
                found += [[l * members + 4 * z + t for t in range(4)] for z in range(pairs)]
        return found

    current = jnp.zeros((SEG, half_width), jnp.bfloat16)
    kept = (jnp.zeros((pairs, 128, 128), jnp.float32),) + (jnp.zeros((pairs, SEG, 128), jnp.bfloat16),) * 2
    finished = []
    near = 4 * HEAD
    for slot in range(sections + 2):
        if slot in (0, 2):
            current = jnp.where(line == 0, entry[slot // 2], current)
        got = lax.all_gather(current, ("pp", "tp"), axis_index_groups=groups(slot))
        after = finished[0] if slot == sections + 1 else ()
        current, *kept = section(slot, got, gain, weights, edge, spike, out_gain, kept, after)
        if slot in (sections - 1, sections + 1):
            unit = len(finished)
            finished.append(
                [
                    between(
                        current[:, part * near : part * near + near],
                        [(sections - 1, 2 * k + unit, 2 * k, 2 * k % 4 + 4 * part) for k in range(micro)],
                    )
                    for part in range(chips // 4)
                ]
            )
    mine = [jnp.where(line % 2 == 0, even, odd) for even, odd in zip(*finished)]
    chip = lax.axis_index("tp") // 2
    held = mine[0]
    for part in range(1, chips // 4):
        held = jnp.where(chip // 4 == part, mine[part], held)
    close = [[8 * part + 2 * z + c for z in range(4)] for part in range(chips // 4) for c in range(2)]
    received = lax.all_gather(held, "tp", axis_index_groups=close)
    received = lax.dynamic_index_in_dim(received, line // 2 * 2 % 4, 0, keepdims=False)
    return lax.dynamic_slice_in_dim(received, chip % 4 * HEAD, HEAD, 1)


def solution(mesh):
    in_specs = (
        P("pp", "tp"),
        P("pp", None),
        P("pp", "tp", None),
        P("pp", "tp", None),
        P("pp", "tp", None),
        P("pp", "tp", None),
        P("pp", "tp"),
        P("pp", None, "tp"),
        P("pp", None),
    )
    out_specs = P("pp", "tp")
    return jax.shard_map(shards, mesh=mesh, in_specs=in_specs, out_specs=out_specs, check_vma=False)
```

```python
import functools

import jax
import jax.numpy as jnp
from jax import lax
from jax.experimental import pallas as pl
from jax.experimental.pallas import tpu as pltpu
from jax.sharding import PartitionSpec as P

HEAD = 64
SEG = 64
EPSILON = 1e-06
NT = (((1,), (1,)), ((), ()))
NN = (((1,), (0,)), ((), ()))
TN = (((0,), (0,)), ((), ()))
ABREAST = 8


def section_kernel(
    slot,
    got,
    gain,
    weights,
    edge,
    spike,
    out_gain,
    state_in,
    keys_in,
    values_in,
    *others,
):
    if slot == 0:
        source = weights
        result, weights, state, last_keys, last_values, scaled, product, semaphores = others
    else:
        result, state, last_keys, last_values, scaled, product = others[-6:]
    line = lax.axis_index("pp")
    core = lax.axis_index("tp") % 2
    first = (line == slot).astype(jnp.int32)
    pairs = weights.shape[0] // 2

    def ready(head):
        if slot == 0:
            pltpu.make_async_copy(source.at[head], weights.at[head], semaphores.at[head]).wait()

    if slot == 0:
        for head in range(2 * pairs):
            pltpu.make_async_copy(source.at[head], weights.at[head], semaphores.at[head]).start()

        @pl.when(line != 0)
        def _():
            for head in range(2 * pairs):
                ready(head)

    @pl.when(line == slot - 1)
    def _():
        at = lax.broadcasted_iota(jnp.int32, (128, 128), 0) < HEAD
        of = lax.broadcasted_iota(jnp.int32, (128, 128), 1) < HEAD
        for pair in range(pairs):
            carried = lax.dot_general(last_keys[pair], last_values[pair], TN, preferred_element_type=jnp.float32)
            state[pair] = jnp.where(at == of, carried, 0.0)

    @pl.when((line == slot) | (line == slot - 2))
    def _():
        run_section(
            first,
            core,
            got,
            gain,
            weights,
            edge,
            spike,
            out_gain,
            result,
            state,
            last_keys,
            last_values,
            scaled,
            product,
            ready,
        )


def run_section(
    first,
    core,
    got,
    gain,
    weights,
    edge,
    spike,
    out_gain,
    result,
    state,
    last_keys,
    last_values,
    scaled,
    product,
    ready,
):
    rows, width = got.shape[1:]
    heads = weights.shape[0]
    low = lax.broadcasted_iota(jnp.int32, (rows, 128), 1) < HEAD

    total = jnp.zeros((rows, 128), jnp.float32)
    for tile in range(width // 128):
        columns = pl.ds(tile * 128, 128)
        even = got[0, :, columns].astype(jnp.float32)
        odd = got[1, :, columns].astype(jnp.float32)
        total = total + even * even + odd * odd
        left = jnp.where(low, even, pltpu.roll(odd, HEAD, 1))
        right = jnp.where(low, pltpu.roll(even, HEAD, 1), odd)
        for step, wide in enumerate((left, right)):
            columns = pl.ds((2 * tile + step) * 128, 128)
            scaled[:, columns] = (wide * gain[:, columns]).astype(jnp.bfloat16)
    total = jnp.sum(total, axis=1, keepdims=True)
    scale = jnp.broadcast_to(lax.rsqrt(total / (2 * width) + EPSILON), (rows, 128))

    at = lax.broadcasted_iota(jnp.int32, (rows, 2 * rows), 0)
    of = lax.broadcasted_iota(jnp.int32, (rows, 2 * rows), 1)
    ones = jnp.where(at >= jnp.where(of >= rows, of - rows, of), 1.0, 0.0).astype(jnp.bfloat16)
    at = lax.broadcasted_iota(jnp.int32, (2 * rows, rows), 0)
    of = lax.broadcasted_iota(jnp.int32, (2 * rows, rows), 1)
    causal = jnp.where(at >= rows, at - rows, at) >= of
    same = (lax.broadcasted_iota(jnp.int32, (128, 128), 0) < HEAD) == (
        lax.broadcasted_iota(jnp.int32, (128, 128), 1) < HEAD
    )
    mean = jnp.where(same, 1.0 / HEAD, 0.0).astype(jnp.bfloat16)

    def multiply(head, _):
        ready(head)
        product[head] = lax.dot_general(scaled[...], weights[head], NN, preferred_element_type=jnp.float32)
        return 0

    lax.fori_loop(0, heads, multiply, 0, unroll=8)

    def several(index, _):
        pairs = [ABREAST * index + step for step in range(ABREAST)]
        queries, keys, forgets, values, gates = [], [], [], [], []
        for pair in pairs:
            tiles = [product[2 * pair + k // 2, :, 128 * (k % 2) : 128 * (k % 2) + 128] * scale for k in range(4)]
            rolled = [pltpu.roll(tile, HEAD, 1) for tile in tiles]
            query_pre = jnp.where(low, tiles[0], rolled[2])
            forget_pre = jnp.where(low, rolled[0], tiles[2])
            gate_pre = jnp.where(low, rolled[1], tiles[3])
            values.append(jnp.where(low, tiles[1], rolled[3]).astype(jnp.bfloat16))
            gates.append(gate_pre * jax.nn.sigmoid(gate_pre) * out_gain[...])
            queries.append(query_pre * jax.nn.sigmoid(query_pre))
            lower = edge[pair]
            upper = 1.0 - lower
            opposite = jnp.exp(jnp.minimum(-forget_pre, 80.0))
            kept = 1.0 / (1.0 + opposite)
            forgets.append(jnp.log(lower + upper * kept) + spike[1 - first, pair])
            keys.append(upper * (opposite * kept))

        running = []
        for step in range(0, ABREAST, 2):
            wide = jnp.concatenate(forgets[step : step + 2], axis=1)
            high = wide.astype(jnp.bfloat16)
            rest = (wide - high.astype(jnp.float32)).astype(jnp.bfloat16)
            wide = lax.dot_general(
                ones, jnp.concatenate([high, rest], axis=0), NN, preferred_element_type=jnp.float32
            )
            running += [wide[:, :128], wide[:, 128:]]

        squares, mixes = [], []
        for step, pair in enumerate(pairs):
            query_scaled = queries[step] * jnp.exp(running[step])
            key_scaled = (keys[step] * jnp.exp(-running[step])).astype(jnp.bfloat16)
            stacked = jnp.concatenate(
                [jnp.where(low, query_scaled, 0.0), jnp.where(low, 0.0, query_scaled)], axis=0
            ).astype(jnp.bfloat16)
            scores = lax.dot_general(stacked, key_scaled, NT, preferred_element_type=jnp.float32)
            scores = jnp.where(causal, scores, 0.0).astype(jnp.bfloat16)
            before = jnp.where(first == 1, 0.0, state[pair]).astype(jnp.bfloat16)
            both = lax.dot_general(
                jnp.concatenate([stacked, scores], axis=1),
                jnp.concatenate([before, values[step]], axis=0),
                NN,
                preferred_element_type=jnp.float32,
            )
            mixed = jnp.where(low, both[:rows], both[rows:])
            mixes.append(mixed)
            squares.append((mixed * mixed).astype(jnp.bfloat16))
            ending = running[step][rows - 1 :, :]
            last_keys[pair] = (keys[step] * jnp.exp(ending - running[step])).astype(jnp.bfloat16)
            last_values[pair] = values[step]

        average = lax.dot_general(
            jnp.concatenate(squares, axis=0), mean, NN, preferred_element_type=jnp.float32
        )
        for step, pair in enumerate(pairs):
            inverse = lax.rsqrt(average[rows * step : rows * step + rows] + EPSILON)
            columns = pl.ds(pl.multiple_of(pair * 128, 128), 128)
            own = got[core, :, columns].astype(jnp.float32)
            result[:, columns] = (own + mixes[step] * inverse * gates[step]).astype(jnp.bfloat16)
        return 0

    lax.fori_loop(0, heads // 2 // ABREAST, several, 0)


def section(slot, got, gain, weights, edge, spike, out_gain, kept, after):
    rows, width = got.shape[1:]
    everything = [pl.BlockSpec(memory_space=pltpu.VMEM)]
    outputs = [jax.ShapeDtypeStruct((rows, width), jnp.bfloat16)]
    scratch = [
        pltpu.VMEM((rows, 2 * width), jnp.bfloat16),
        pltpu.VMEM((weights.shape[0], rows, weights.shape[2]), jnp.float32),
    ]
    source = everything
    if slot == 0:
        source = [pl.BlockSpec(memory_space=pltpu.HBM)]
        weights = pltpu.with_memory_space_constraint(weights, pltpu.HBM)
        outputs.append(pltpu.VMEM(weights.shape, weights.dtype))
        scratch.append(pltpu.SemaphoreType.DMA((weights.shape[0],)))
    results = pl.pallas_call(
        functools.partial(section_kernel, slot),
        out_shape=outputs + [jax.ShapeDtypeStruct(array.shape, array.dtype) for array in kept],
        in_specs=everything * 2 + source + everything * (6 + len(after)),
        out_specs=everything * (len(outputs) + 3),
        scratch_shapes=scratch,
        input_output_aliases={6 + index: len(outputs) + index for index in range(3)},
        compiler_params=pltpu.CompilerParams(vmem_limit_bytes=24 << 20),
        cost_estimate=pl.CostEstimate(
            flops=2 * rows * weights.size, bytes_accessed=2 * weights.size, transcendentals=0
        ),
    )(got, gain, weights, edge, spike, out_gain, *kept, *after)
    held = results[1] if slot == 0 else weights
    return results[0], held, results[-3:]


def shards(
    entry_stream_rows,
    layer_rescale_factor,
    probe_projection,
    retention_projection,
    candidate_projection,
    emission_filter_matrix,
    retention_minimum,
    decay_spike,
    per_group_scale,
):
    sections = lax.axis_size("pp")
    members = lax.axis_size("tp")
    chips = members // 2
    line = lax.axis_index("pp")
    half_width = layer_rescale_factor.shape[1] // 2
    pairs = chips // 2
    same_core = [[c + 2 * z for z in range(chips)] for c in range(2)]

    local = jnp.stack(
        [probe_projection[0], retention_projection[0], candidate_projection[0], emission_filter_matrix[0]]
    )
    local = local.reshape(4 * HEAD, 2 * half_width).T
    weights = lax.all_gather(local, "tp", axis_index_groups=same_core)
    gain = layer_rescale_factor
    out_gain = jnp.tile(per_group_scale, (1, 2))
    rest = jnp.concatenate([retention_minimum[0], decay_spike[0, :, 0]])
    parts = []
    for _ in range(3):
        part = lax.reduce_precision(rest, 8, 7)
        parts.append(part.astype(jnp.bfloat16))
        rest = rest - part
    parts = jnp.concatenate(parts).reshape(-1, HEAD)
    extra = parts.shape[0]
    padding = jnp.zeros((16 - extra, HEAD), jnp.bfloat16)
    whole = lax.all_gather(
        jnp.concatenate([entry_stream_rows, parts, padding]), "tp", axis_index_groups=same_core
    )
    entering = whole[:, :SEG].transpose(1, 0, 2).reshape(SEG, half_width)
    small = whole[:, SEG : SEG + extra].astype(jnp.float32).reshape(chips, 3, 3 * HEAD).sum(axis=1)
    edge = small[:, :HEAD].reshape(pairs, 1, 128)
    spike = small[:, HEAD:].reshape(pairs, 2, 2, SEG)
    spike = jnp.broadcast_to(spike.transpose(2, 0, 3, 1)[..., None], (2, pairs, SEG, 2, HEAD))
    spike = spike.reshape(2, pairs, SEG, 128)
    gain, out_gain, edge, spike = lax.optimization_barrier((gain, out_gain, edge, spike))

    def between(array, pairs_of):
        moves = [
            (a * members + 2 * z + c, b * members + 2 * y + c) for a, b, z, y in pairs_of for c in range(2)
        ]
        return lax.ppermute(array, ("pp", "tp"), moves)

    micro = sections // 2
    entry = [between(entering, [(2 * k + u, 0, 2 * k, 2 * k) for k in range(micro)]) for u in range(2)]

    def groups(slot):
        paired, found = set(), []
        for unit in range(2):
            a, b = slot - 2 * unit - 1, slot - 2 * unit
            if a >= 0 and b < sections:
                paired |= {a, b}
                found += [[l * members + 2 * z + c for l in (a, b) for c in range(2)] for z in range(chips)]
        for l in range(sections):
            if l not in paired:
                found += [[l * members + 4 * z + t for t in range(4)] for z in range(pairs)]
        return found

    current = jnp.zeros((SEG, half_width), jnp.bfloat16)
    kept = (jnp.zeros((pairs, 128, 128), jnp.float32),) + (jnp.zeros((pairs, SEG, 128), jnp.bfloat16),) * 2
    finished = []
    near = 4 * HEAD
    for slot in range(sections + 2):
        if slot in (0, 2):
            current = jnp.where(line == 0, entry[slot // 2], current)
        got = lax.all_gather(current, ("pp", "tp"), axis_index_groups=groups(slot))
        after = finished[0] if slot == sections + 1 else ()
        current, weights, kept = section(slot, got, gain, weights, edge, spike, out_gain, kept, after)
        if slot in (sections - 1, sections + 1):
            unit = len(finished)
            finished.append(
                [
                    between(
                        current[:, part * near : part * near + near],
                        [(sections - 1, 2 * k + unit, 2 * k, 2 * k % 4 + 4 * part) for k in range(micro)],
                    )
                    for part in range(chips // 4)
                ]
            )
    mine = [jnp.where(line % 2 == 0, even, odd) for even, odd in zip(*finished)]
    chip = lax.axis_index("tp") // 2
    held = mine[0]
    for part in range(1, chips // 4):
        held = jnp.where(chip // 4 == part, mine[part], held)
    origin = line // 2 * 2 % 4

    def chunk(index):
        return lax.dynamic_slice_in_dim(held, index * HEAD, HEAD, 1)

    out = jnp.where(chip % 4 == origin, chunk(origin), 0)
    for flip in range(1, 4):
        moves = [
            (l * members + 8 * part + 2 * at + c, l * members + 8 * part + 2 * (at ^ flip) + c)
            for l in range(sections)
            for at in [l // 2 * 2 % 4]
            for part in range(chips // 4)
            for c in range(2)
        ]
        out = out + lax.ppermute(chunk(origin ^ flip), ("pp", "tp"), moves)
    return out


def solution(mesh):
    in_specs = (
        P("pp", "tp"),
        P("pp", None),
        P("pp", "tp", None),
        P("pp", "tp", None),
        P("pp", "tp", None),
        P("pp", "tp", None),
        P("pp", "tp"),
        P("pp", None, "tp"),
        P("pp", None),
    )
    out_specs = P("pp", "tp")
    return jax.shard_map(shards, mesh=mesh, in_specs=in_specs, out_specs=out_specs, check_vma=False)
```

```python
import functools

import jax
import jax.numpy as jnp
from jax import lax
from jax.experimental import pallas as pl
from jax.experimental.pallas import tpu as pltpu
from jax.sharding import PartitionSpec as P

HEAD = 64
SEG = 64
EPSILON = 1e-06
NT = (((1,), (1,)), ((), ()))
NN = (((1,), (0,)), ((), ()))
TN = (((0,), (0,)), ((), ()))
ABREAST = 8


def section_kernel(
    slot,
    got,
    gain,
    weights,
    edge,
    spike,
    out_gain,
    state_in,
    keys_in,
    values_in,
    *others,
):
    if slot == 0:
        source = weights
        result, weights, state, last_keys, last_values, scaled, product, semaphores = others
    else:
        result, state, last_keys, last_values, scaled, product = others[-6:]
    line = lax.axis_index("pp")
    core = lax.axis_index("tp") % 2
    first = (line == slot).astype(jnp.int32)
    pairs = weights.shape[0] // 2

    def ready(head):
        if slot == 0:
            pltpu.make_async_copy(source.at[head], weights.at[head], semaphores.at[head]).wait()

    if slot == 0:
        for head in range(2 * pairs):
            pltpu.make_async_copy(source.at[head], weights.at[head], semaphores.at[head]).start()

        @pl.when(line != 0)
        def _():
            for head in range(2 * pairs):
                ready(head)

    @pl.when(line == slot - 1)
    def _():
        at = lax.broadcasted_iota(jnp.int32, (128, 128), 0) < HEAD
        of = lax.broadcasted_iota(jnp.int32, (128, 128), 1) < HEAD
        for pair in range(pairs):
            carried = lax.dot_general(last_keys[pair], last_values[pair], TN, preferred_element_type=jnp.float32)
            state[pair] = jnp.where(at == of, carried, 0.0)

    @pl.when((line == slot) | (line == slot - 2))
    def _():
        run_section(
            first,
            core,
            got,
            gain,
            weights,
            edge,
            spike,
            out_gain,
            result,
            state,
            last_keys,
            last_values,
            scaled,
            product,
            ready,
        )


def run_section(
    first,
    core,
    got,
    gain,
    weights,
    edge,
    spike,
    out_gain,
    result,
    state,
    last_keys,
    last_values,
    scaled,
    product,
    ready,
):
    rows, width = got.shape[1:]
    heads = weights.shape[0]
    low = lax.broadcasted_iota(jnp.int32, (rows, 128), 1) < HEAD

    total = jnp.zeros((rows, 128), jnp.float32)
    for tile in range(width // 128):
        columns = pl.ds(tile * 128, 128)
        even = got[0, :, columns].astype(jnp.float32)
        odd = got[1, :, columns].astype(jnp.float32)
        total = total + even * even + odd * odd
        left = jnp.where(low, even, pltpu.roll(odd, HEAD, 1))
        right = jnp.where(low, pltpu.roll(even, HEAD, 1), odd)
        for step, wide in enumerate((left, right)):
            columns = pl.ds((2 * tile + step) * 128, 128)
            scaled[:, columns] = (wide * gain[:, columns]).astype(jnp.bfloat16)
    total = jnp.sum(total, axis=1, keepdims=True)
    scale = jnp.broadcast_to(lax.rsqrt(total / (2 * width) + EPSILON), (rows, 128))

    at = lax.broadcasted_iota(jnp.int32, (rows, 2 * rows), 0)
    of = lax.broadcasted_iota(jnp.int32, (rows, 2 * rows), 1)
    ones = jnp.where(at >= jnp.where(of >= rows, of - rows, of), 1.0, 0.0).astype(jnp.bfloat16)
    at = lax.broadcasted_iota(jnp.int32, (2 * rows, rows), 0)
    of = lax.broadcasted_iota(jnp.int32, (2 * rows, rows), 1)
    causal = jnp.where(at >= rows, at - rows, at) >= of
    same = (lax.broadcasted_iota(jnp.int32, (128, 128), 0) < HEAD) == (
        lax.broadcasted_iota(jnp.int32, (128, 128), 1) < HEAD
    )
    mean = jnp.where(same, 1.0 / HEAD, 0.0).astype(jnp.bfloat16)

    def multiply(head, _):
        ready(head)
        product[head] = lax.dot_general(scaled[...], weights[head], NN, preferred_element_type=jnp.float32)
        return 0

    for head in range(heads):
        multiply(head, 0)

    def several(index, _):
        pairs = [ABREAST * index + step for step in range(ABREAST)]
        queries, keys, forgets, values, gates = [], [], [], [], []
        for pair in pairs:
            tiles = [product[2 * pair + k // 2, :, 128 * (k % 2) : 128 * (k % 2) + 128] * scale for k in range(4)]
            rolled = [pltpu.roll(tile, HEAD, 1) for tile in tiles]
            query_pre = jnp.where(low, tiles[0], rolled[2])
            forget_pre = jnp.where(low, rolled[0], tiles[2])
            gate_pre = jnp.where(low, rolled[1], tiles[3])
            values.append(jnp.where(low, tiles[1], rolled[3]).astype(jnp.bfloat16))
            gates.append(gate_pre * jax.nn.sigmoid(gate_pre) * out_gain[...])
            queries.append(query_pre * jax.nn.sigmoid(query_pre))
            lower = edge[pair]
            upper = 1.0 - lower
            opposite = jnp.exp(jnp.minimum(-forget_pre, 80.0))
            kept = 1.0 / (1.0 + opposite)
            forgets.append(jnp.log(lower + upper * kept) + spike[1 - first, pair])
            keys.append(upper * (opposite * kept))

        running = []
        for step in range(0, ABREAST, 2):
            wide = jnp.concatenate(forgets[step : step + 2], axis=1)
            high = wide.astype(jnp.bfloat16)
            rest = (wide - high.astype(jnp.float32)).astype(jnp.bfloat16)
            wide = lax.dot_general(
                ones, jnp.concatenate([high, rest], axis=0), NN, preferred_element_type=jnp.float32
            )
            running += [wide[:, :128], wide[:, 128:]]

        squares, mixes = [], []
        for step, pair in enumerate(pairs):
            query_scaled = queries[step] * jnp.exp(running[step])
            key_scaled = (keys[step] * jnp.exp(-running[step])).astype(jnp.bfloat16)
            stacked = jnp.concatenate(
                [jnp.where(low, query_scaled, 0.0), jnp.where(low, 0.0, query_scaled)], axis=0
            ).astype(jnp.bfloat16)
            scores = lax.dot_general(stacked, key_scaled, NT, preferred_element_type=jnp.float32)
            scores = jnp.where(causal, scores, 0.0).astype(jnp.bfloat16)
            before = jnp.where(first == 1, 0.0, state[pair]).astype(jnp.bfloat16)
            both = lax.dot_general(
                jnp.concatenate([stacked, scores], axis=1),
                jnp.concatenate([before, values[step]], axis=0),
                NN,
                preferred_element_type=jnp.float32,
            )
            mixed = jnp.where(low, both[:rows], both[rows:])
            mixes.append(mixed)
            squares.append((mixed * mixed).astype(jnp.bfloat16))
            ending = running[step][rows - 1 :, :]
            last_keys[pair] = (keys[step] * jnp.exp(ending - running[step])).astype(jnp.bfloat16)
            last_values[pair] = values[step]

        average = lax.dot_general(
            jnp.concatenate(squares, axis=0), mean, NN, preferred_element_type=jnp.float32
        )
        for step, pair in enumerate(pairs):
            inverse = lax.rsqrt(average[rows * step : rows * step + rows] + EPSILON)
            columns = pl.ds(pl.multiple_of(pair * 128, 128), 128)
            own = got[core, :, columns].astype(jnp.float32)
            result[:, columns] = (own + mixes[step] * inverse * gates[step]).astype(jnp.bfloat16)
        return 0

    for index in range(heads // 2 // ABREAST):
        several(index, 0)


def section(slot, got, gain, weights, edge, spike, out_gain, kept, after):
    rows, width = got.shape[1:]
    everything = [pl.BlockSpec(memory_space=pltpu.VMEM)]
    outputs = [jax.ShapeDtypeStruct((rows, width), jnp.bfloat16)]
    scratch = [
        pltpu.VMEM((rows, 2 * width), jnp.bfloat16),
        pltpu.VMEM((weights.shape[0], rows, weights.shape[2]), jnp.float32),
    ]
    source = everything
    if slot == 0:
        source = [pl.BlockSpec(memory_space=pltpu.HBM)]
        weights = pltpu.with_memory_space_constraint(weights, pltpu.HBM)
        outputs.append(pltpu.VMEM(weights.shape, weights.dtype))
        scratch.append(pltpu.SemaphoreType.DMA((weights.shape[0],)))
    results = pl.pallas_call(
        functools.partial(section_kernel, slot),
        out_shape=outputs + [jax.ShapeDtypeStruct(array.shape, array.dtype) for array in kept],
        in_specs=everything * 2 + source + everything * (6 + len(after)),
        out_specs=everything * (len(outputs) + 3),
        scratch_shapes=scratch,
        input_output_aliases={6 + index: len(outputs) + index for index in range(3)},
        compiler_params=pltpu.CompilerParams(vmem_limit_bytes=24 << 20),
        cost_estimate=pl.CostEstimate(
            flops=2 * rows * weights.size, bytes_accessed=2 * weights.size, transcendentals=0
        ),
    )(got, gain, weights, edge, spike, out_gain, *kept, *after)
    held = results[1] if slot == 0 else weights
    return results[0], held, results[-3:]


def shards(
    entry_stream_rows,
    layer_rescale_factor,
    probe_projection,
    retention_projection,
    candidate_projection,
    emission_filter_matrix,
    retention_minimum,
    decay_spike,
    per_group_scale,
):
    sections = lax.axis_size("pp")
    members = lax.axis_size("tp")
    chips = members // 2
    line = lax.axis_index("pp")
    half_width = layer_rescale_factor.shape[1] // 2
    pairs = chips // 2
    same_core = [[c + 2 * z for z in range(chips)] for c in range(2)]

    local = jnp.stack(
        [probe_projection[0], retention_projection[0], candidate_projection[0], emission_filter_matrix[0]]
    )
    local = local.reshape(4 * HEAD, 2 * half_width).T
    weights = lax.all_gather(local, "tp", axis_index_groups=same_core)
    gain = layer_rescale_factor
    out_gain = jnp.tile(per_group_scale, (1, 2))
    rest = jnp.concatenate([retention_minimum[0], decay_spike[0, :, 0]])
    parts = []
    for _ in range(3):
        part = lax.reduce_precision(rest, 8, 7)
        parts.append(part.astype(jnp.bfloat16))
        rest = rest - part
    parts = jnp.concatenate(parts).reshape(-1, HEAD)
    extra = parts.shape[0]
    padding = jnp.zeros((16 - extra, HEAD), jnp.bfloat16)
    whole = lax.all_gather(
        jnp.concatenate([entry_stream_rows, parts, padding]), "tp", axis_index_groups=same_core
    )
    entering = whole[:, :SEG].transpose(1, 0, 2).reshape(SEG, half_width)
    small = whole[:, SEG : SEG + extra].astype(jnp.float32).reshape(chips, 3, 3 * HEAD).sum(axis=1)
    edge = small[:, :HEAD].reshape(pairs, 1, 128)
    spike = small[:, HEAD:].reshape(pairs, 2, 2, SEG)
    spike = jnp.broadcast_to(spike.transpose(2, 0, 3, 1)[..., None], (2, pairs, SEG, 2, HEAD))
    spike = spike.reshape(2, pairs, SEG, 128)
    gain, out_gain, edge, spike = lax.optimization_barrier((gain, out_gain, edge, spike))

    def between(array, pairs_of):
        moves = [
            (a * members + 2 * z + c, b * members + 2 * y + c) for a, b, z, y in pairs_of for c in range(2)
        ]
        return lax.ppermute(array, ("pp", "tp"), moves)

    micro = sections // 2
    entry = [between(entering, [(2 * k + u, 0, 2 * k, 2 * k) for k in range(micro)]) for u in range(2)]

    def groups(slot):
        paired, found = set(), []
        for unit in range(2):
            a, b = slot - 2 * unit - 1, slot - 2 * unit
            if a >= 0 and b < sections:
                paired |= {a, b}
                found += [[l * members + 2 * z + c for l in (a, b) for c in range(2)] for z in range(chips)]
        for l in range(sections):
            if l not in paired:
                found += [[l * members + 4 * z + t for t in range(4)] for z in range(pairs)]
        return found

    current = jnp.zeros((SEG, half_width), jnp.bfloat16)
    kept = (jnp.zeros((pairs, 128, 128), jnp.float32),) + (jnp.zeros((pairs, SEG, 128), jnp.bfloat16),) * 2
    finished = []
    near = 4 * HEAD
    for slot in range(sections + 2):
        if slot in (0, 2):
            current = jnp.where(line == 0, entry[slot // 2], current)
        got = lax.all_gather(current, ("pp", "tp"), axis_index_groups=groups(slot))
        after = finished[0] if slot == sections + 1 else ()
        current, weights, kept = section(slot, got, gain, weights, edge, spike, out_gain, kept, after)
        if slot in (sections - 1, sections + 1):
            unit = len(finished)
            finished.append(
                [
                    between(
                        current[:, part * near : part * near + near],
                        [(sections - 1, 2 * k + unit, 2 * k, 2 * k % 4 + 4 * part) for k in range(micro)],
                    )
                    for part in range(chips // 4)
                ]
            )
    mine = [jnp.where(line % 2 == 0, even, odd) for even, odd in zip(*finished)]
    chip = lax.axis_index("tp") // 2
    held = mine[0]
    for part in range(1, chips // 4):
        held = jnp.where(chip // 4 == part, mine[part], held)
    origin = line // 2 * 2 % 4

    def chunk(index):
        return lax.dynamic_slice_in_dim(held, index * HEAD, HEAD, 1)

    out = jnp.where(chip % 4 == origin, chunk(origin), 0)
    for flip in range(1, 4):
        moves = [
            (l * members + 8 * part + 2 * at + c, l * members + 8 * part + 2 * (at ^ flip) + c)
            for l in range(sections)
            for at in [l // 2 * 2 % 4]
            for part in range(chips // 4)
            for c in range(2)
        ]
        out = out + lax.ppermute(chunk(origin ^ flip), ("pp", "tp"), moves)
    return out


def solution(mesh):
    in_specs = (
        P("pp", "tp"),
        P("pp", None),
        P("pp", "tp", None),
        P("pp", "tp", None),
        P("pp", "tp", None),
        P("pp", "tp", None),
        P("pp", "tp"),
        P("pp", None, "tp"),
        P("pp", None),
    )
    out_specs = P("pp", "tp")
    return jax.shard_map(shards, mesh=mesh, in_specs=in_specs, out_specs=out_specs, check_vma=False)
```
